32 devices in a mesh: st: 16 (over z, y, x), tp: 2 (over core).
Axes of the slice: x: 2, y: 2, z: 4, core: 2. Of those that a mesh axis runs over, the one named last changes fastest.
Arguments:
- tokens: bfloat16 [12288, 2048], P('st'), may hold values from -6 to 6, as said below
- route_ids: int32 [192, 4], P('st'), may hold values from 0 to 383, as said below
- store: bfloat16 [384, 128, 2048], P('st'), may hold values from -6 to 6, as said below
- token_gain: float32 [2048], replicated, may hold values from 0.1 to 1.9
- store_gain: float32 [2048], replicated, may hold values from 0.1 to 1.9
- carry_weight: bfloat16 [2048, 512], P(None, 'tp'), may hold values from -0.125 to 0.125
- spatial_weight: bfloat16 [2048, 512], P(None, 'tp'), may hold values from -0.125 to 0.125
- spatial_gain: float32 [512], P('tp'), may hold values from 0.1 to 1.9
- position_mix: bfloat16 [8, 128, 128], P('tp'), may hold values from -0.5 to 0.5
- position_bias: float32 [8, 128], P('tp'), may hold values from 0.1 to 1.9
- query_weight: bfloat16 [2048, 512], P(None, 'tp'), may hold values from -0.86178639 to 0.86178639, as said below
- key_weight: bfloat16 [2048, 512], P(None, 'tp'), may hold values from -0.86178639 to 0.86178639, as said below
- read_weight: bfloat16 [2048, 512], P(None, 'tp'), may hold values from -0.125 to 0.125
- blend_weight: bfloat16 [2048, 512], P(None, 'tp'), may hold values from -0.125 to 0.125
- output_weight: bfloat16 [512, 2048], replicated, may hold values from -0.25 to 0.25
Outputs:
- mixed: bfloat16 [12288, 2048], P(('st', 'tp'))
The draws below stay inside these ranges and needn't reach their ends.
Inputs may be any that keep to these rules, and one draw needn't show every extreme that they name: `route_ids`: each entry is a passage index; passage p is held by index p // 24 of st. All entries of the spans of one index of st (aligned blocks of 12 rows) are different; they name at most 6 passage held by any one index of st, exactly 6 held by the index before their own (cyclically), and at least one held by the index half the axis away. `tokens`: Activations; in some draws the first token of some spans equals a row of a passage that the span reads. `store`: passage rows. `query_weight`: A projection matrix. `key_weight`: A projection matrix.
All inputs are finite; a program needn't handle non-finite values.
Results may differ from the reference program's by a relative error of at most 0.012.
The reference program's roundings to bfloat16 on the way count: a program that leaves them out, or rounds other values in their place, can miss the bound.
Values may be sent and summed in bfloat16 or wider, within the bound.
A program may use at most 128 MiB of HBM per device.

```python
import jax
import jax.numpy as jnp
from jax import lax

D = 2048
HEADS = 8
HEAD_DIM = 64
WIDTH = 512
BLOCK = 128
SPAN = 64
PICKS = 4
PASS_ROWS = 128
PASS_DEV = 24
TOK_DEV = 768
TOKENS = 12288
PASSAGES = 384
CAP = 6
N_ST = 16


def store_passage(key, passage):
    passage_key = jax.random.fold_in(jax.random.fold_in(key, 5), passage)
    sample = jax.random.normal(passage_key, (PASS_ROWS, D), jnp.float32)
    return jnp.clip(sample, -6.0, 6.0)


def draw_store(key, part):
    indices = jnp.arange(PASSAGES, dtype=jnp.int32)
    return lax.map(lambda passage: store_passage(key, passage).astype(jnp.bfloat16), indices)


def route_table(key):
    base_key = jax.random.fold_in(key, 3)
    span_dev = TOK_DEV // SPAN
    wanted = span_dev * PICKS
    pool_size = N_ST * CAP
    ranks = jax.random.permutation(jax.random.fold_in(base_key, 0), N_ST)
    heat = 1 + ranks % 4
    slots = jnp.arange(pool_size, dtype=jnp.int32)
    slot_owner = slots // CAP
    slot_copy = slots % CAP

    def reader(index):
        subkeys = jax.random.split(jax.random.fold_in(base_key, index + 1), 3)
        raw_score = jax.random.randint(subkeys[0], (pool_size,), 0, 4096, dtype=jnp.int32)
        score = raw_score * heat[slot_owner] * pool_size + slots
        before = (index + N_ST - 1) % N_ST
        across = (index + N_ST // 2) % N_ST
        forced = (slot_owner == before) | (slot_owner == across) & (slot_copy == 0)
        score = jnp.where(forced, slots - pool_size, score)
        chosen = jnp.argsort(score)[:wanted]
        owner_index = slot_owner[chosen]
        offset = jax.random.randint(subkeys[1], (N_ST,), 0, PASS_DEV, dtype=jnp.int32)
        passage = owner_index * PASS_DEV + (offset[owner_index] + slot_copy[chosen]) % PASS_DEV
        shuffle = jax.random.permutation(subkeys[2], wanted)
        return passage[shuffle].reshape(span_dev, PICKS)
    table = lax.map(reader, jnp.arange(N_ST, dtype=jnp.int32))
    return table.reshape(N_ST * span_dev, PICKS).astype(jnp.int32)


def draw_route_ids(key, part):
    return route_table(key)


def draw_tokens(key, part):
    sample = jnp.clip(jax.random.normal(jax.random.fold_in(key, 9), (TOKENS, D), jnp.float32), -6.0, 6.0)
    return sample.astype(jnp.bfloat16)


def query_key_pair(key):
    base_key = jax.random.fold_in(key, 13)
    first = jnp.clip(jax.random.normal(jax.random.fold_in(base_key, 0), (D, WIDTH), jnp.float32), -6.0, 6.0)
    second = jnp.clip(jax.random.normal(jax.random.fold_in(base_key, 1), (D, WIDTH), jnp.float32), -6.0, 6.0)
    first = first * D ** (-0.5)
    second = second * D ** (-0.5)
    return (first, second)


def draw_query_weight(key, part):
    return query_key_pair(key)[0].astype(jnp.bfloat16)


def draw_key_weight(key, part):
    return query_key_pair(key)[1].astype(jnp.bfloat16)


def level_of(rng, dims, cuts, least, high):
    factor_of, own = 1.0, jax.random.fold_in(rng, 6)
    for position, blocks in cuts:
        heights = jnp.exp(jax.random.uniform(jax.random.fold_in(own, position), (blocks,), jnp.float32, least / len(cuts), high / len(cuts)))
        factor_of = factor_of * jnp.repeat(heights, dims[position] // blocks).reshape([-1 if axis == position else 1 for axis in range(len(dims))])
    return factor_of


def noise(rng, extent, deviation, most, cuts=(), held_as=jnp.bfloat16):
    drawn = jax.random.normal(rng, extent, jnp.float32) * deviation
    if len(cuts) > 0:
        drawn = level_of(rng, extent, cuts, -0.22, 0.18) * drawn
    return jnp.clip(drawn, min=-most, max=most).astype(held_as)


def setup_inputs(seed: int = 0) -> dict:
    streams_of = jax.random.split(jax.random.key(seed), 16)
    tokens = draw_tokens(jax.random.fold_in(streams_of[15], 71), 0)
    route_ids = draw_route_ids(jax.random.fold_in(streams_of[15], 71), 0)
    store = draw_store(jax.random.fold_in(streams_of[15], 71), 0)
    token_gain = jnp.clip(1.0 + 0.18 * jax.random.normal(streams_of[3], (D,), jnp.float32), 0.1, 1.9)
    store_gain = jnp.clip(1.0 + 0.18 * jax.random.normal(streams_of[4], (D,), jnp.float32), 0.1, 1.9)
    carry_weight = noise(streams_of[5], (D, WIDTH), D ** -0.5, 0.125, ((1, 2),))
    spatial_weight = noise(streams_of[6], (D, WIDTH), D ** -0.5, 0.125, ((1, 2),))
    spatial_gain = jnp.clip(1.0 + 0.18 * jax.random.normal(streams_of[7], (WIDTH,), jnp.float32), 0.1, 1.9)
    position_mix = noise(streams_of[8], (HEADS, BLOCK, BLOCK), BLOCK ** -0.5, 0.5, ((0, 2),))
    position_bias = jnp.clip(1.0 + 0.18 * jax.random.normal(streams_of[9], (HEADS, BLOCK), jnp.float32), 0.1, 1.9)
    query_weight = draw_query_weight(jax.random.fold_in(streams_of[15], 71), 0)
    key_weight = draw_key_weight(jax.random.fold_in(streams_of[15], 71), 0)
    read_weight = noise(streams_of[12], (D, WIDTH), D ** -0.5, 0.125, ((1, 2),))
    blend_weight = noise(streams_of[13], (D, WIDTH), D ** -0.5, 0.125, ((1, 2),))
    output_weight = noise(streams_of[14], (WIDTH, D), WIDTH ** -0.5, 0.25)
    return dict(tokens=tokens, route_ids=route_ids, store=store, token_gain=token_gain, store_gain=store_gain, carry_weight=carry_weight, spatial_weight=spatial_weight, spatial_gain=spatial_gain, position_mix=position_mix, position_bias=position_bias, query_weight=query_weight, key_weight=key_weight, read_weight=read_weight, blend_weight=blend_weight, output_weight=output_weight)


norm_eps = 1e-06

def rms_scaled(matrix, gain_vector):
    values = matrix.astype(jnp.float32)
    scaled = values * lax.rsqrt(lax.optimization_barrier(jnp.mean(values * values, axis=-1, keepdims=True)) + norm_eps)
    return (scaled * gain_vector.astype(jnp.float32)).astype(jnp.bfloat16)

def passage_partial(queries, key_rows, value_rows):
    score_scale = queries.shape[-1] ** (-0.5)
    scores = jnp.einsum('bthe,bplhe->bpthl', queries.astype(jnp.float32), key_rows.astype(jnp.float32)) * score_scale
    score_peak = lax.optimization_barrier(jnp.max(scores, axis=-1, keepdims=True))
    weights = jnp.exp(scores - score_peak)
    weight_total = lax.optimization_barrier(jnp.sum(weights, axis=-1))
    rounded = lax.optimization_barrier(weights.astype(jnp.bfloat16)).astype(jnp.float32)
    summed = jnp.einsum('bpthl,bplhe->bpthe', rounded, value_rows.astype(jnp.float32))
    partial_value = (summed / weight_total[..., None]).astype(jnp.bfloat16)
    return (partial_value, score_peak[..., 0] + jnp.log(weight_total))

def merge_partials(partial_value, log_total):
    level_top = lax.optimization_barrier(jnp.max(log_total, axis=1, keepdims=True))
    weights = jnp.exp(log_total - level_top)
    weight_total = lax.optimization_barrier(jnp.sum(weights, axis=1))
    summed = lax.optimization_barrier(jnp.sum(weights[..., None] * partial_value.astype(jnp.float32), axis=1))
    return summed / weight_total[..., None]

def reference(tokens, route_ids, store, token_gain, store_gain, carry_weight, spatial_weight, spatial_gain, position_mix, position_bias, query_weight, key_weight, read_weight, blend_weight, output_weight):
    row_count = tokens.shape[0]
    normed = rms_scaled(tokens, token_gain)
    carry_branch = jnp.dot(normed, carry_weight, preferred_element_type=jnp.float32)
    spatial = jax.nn.gelu(jnp.dot(normed, spatial_weight, preferred_element_type=jnp.float32), approximate=False)
    channel_mean = lax.optimization_barrier(jnp.mean(spatial, axis=-1, keepdims=True))
    channel_spread = lax.optimization_barrier(jnp.mean(spatial * spatial, axis=-1, keepdims=True)) - channel_mean * channel_mean
    spatial_in = ((spatial - channel_mean) * lax.rsqrt(channel_spread + norm_eps) * spatial_gain.astype(jnp.float32)).astype(jnp.bfloat16)
    blocks = spatial_in.reshape(row_count // BLOCK, BLOCK, HEADS, HEAD_DIM)
    mixed_blocks = jnp.einsum('hij,njhc->nihc', position_mix.astype(jnp.float32), blocks.astype(jnp.float32))
    mixed_blocks = mixed_blocks + position_bias.astype(jnp.float32).T[None, :, :, None]
    gated_mix = jax.nn.gelu(carry_branch, approximate=False) * mixed_blocks.reshape(row_count, HEADS * HEAD_DIM)

    def project(passage):
        passage_normed = rms_scaled(passage, store_gain)
        return (jnp.dot(passage_normed, key_weight, preferred_element_type=jnp.float32).astype(jnp.bfloat16), jnp.dot(passage_normed, read_weight, preferred_element_type=jnp.float32).astype(jnp.bfloat16))
    store_keys, store_values = lax.map(project, store)
    store_keys = store_keys.reshape(store.shape[0], PASS_ROWS, HEADS, HEAD_DIM)
    store_values = store_values.reshape(store.shape[0], PASS_ROWS, HEADS, HEAD_DIM)
    queries = jnp.dot(normed, query_weight, preferred_element_type=jnp.float32).astype(jnp.bfloat16)
    queries = queries.reshape(row_count // SPAN, SPAN, HEADS, HEAD_DIM)

    def attend(item):
        span_queries, picked = item
        span_keys = store_keys[picked][None]
        span_values = store_values[picked][None]
        partial_value, log_total = passage_partial(span_queries[None], span_keys, span_values)
        return merge_partials(partial_value, log_total)[0]
    memory = lax.map(attend, (queries, route_ids)).reshape(row_count, HEADS * HEAD_DIM)
    blend_gate = jax.nn.sigmoid(jnp.dot(normed, blend_weight, preferred_element_type=jnp.float32))
    mixed_rows = (gated_mix + blend_gate * memory).astype(jnp.bfloat16)
    return jnp.dot(mixed_rows, output_weight, preferred_element_type=jnp.float32).astype(jnp.bfloat16)
```

```python
import functools

import jax
import jax.numpy as jnp
from jax import lax
from jax.experimental import pallas as pl
from jax.experimental.pallas import tpu as pltpu
from jax.sharding import PartitionSpec as P

norm_eps = 1e-06
bf16 = jnp.bfloat16
f32 = jnp.float32


def normed_rows(matrix, gain):
    values = matrix.astype(f32)
    scaled = values * lax.rsqrt(jnp.mean(values * values, axis=-1, keepdims=True) + norm_eps)
    return (scaled * gain).astype(bf16)

far = -1e30
MESH = pl.DeviceIdType.MESH


def query_kernel(span_length, tok_ref, gain_ref, wq_ref, normed_ref, q_ref):
    normed = normed_rows(tok_ref[...], gain_ref[...])
    normed_ref[...] = normed
    q = jnp.dot(normed, wq_ref[...], preferred_element_type=f32).astype(bf16)
    q_ref[...] = q.reshape(q_ref.shape)


def store_kernel(st_ref, gain_ref, wk_ref, wv_ref, k_ref, vt_ref):
    count, length, _ = st_ref.shape
    for p in range(count):
        normed = normed_rows(st_ref[p], gain_ref[...])
        k_ref[p] = jnp.dot(normed, wk_ref[...], preferred_element_type=f32).astype(bf16)
        v = jnp.dot(normed, wv_ref[...], preferred_element_type=f32)
        vt_ref[p] = v.T.astype(bf16)


def stacked_queries(q, heads):
    length, width = q.shape
    dim = width // heads
    row_head = lax.broadcasted_iota(jnp.int32, (heads * length, width), 0) // length
    lane_head = lax.broadcasted_iota(jnp.int32, (heads * length, width), 1) // dim
    return jnp.where(row_head == lane_head, jnp.concatenate([q] * heads, axis=0), jnp.zeros((), bf16))


def own_head(o, heads):
    width, columns = o.shape
    dim, length = width // heads, columns // heads
    col_head = lax.broadcasted_iota(jnp.int32, (dim, columns), 1) // length
    out = o[0:dim]
    for h in range(1, heads):
        out = jnp.where(col_head == h, o[h * dim : (h + 1) * dim], out)
    return out


def route_kernel(
    sizes,
    own_tab,
    tab_ref,
    q_ref,
    k_ref,
    vt_ref,
    gated_ref,
    blend_ref,
    out_ref,
    tabs_v,
    tabs_s,
    qcol,
    qout,
    qin,
    rout,
    lout,
    rin,
    lin,
    mout,
    mlout,
    mid,
    mlin,
    half,
    s_scr,
    w_scr,
    tab_send,
    tab_recv,
    loc,
    ring_send,
    ring_recv,
    qs,
    qr,
    rs,
    rr,
    ls,
    lr,
    ms,
    mr,
    mls,
    mlr,
    ts,
    tr,
):
    columns, plane, parts, heads, cap, picks = sizes
    n = columns * plane
    spans, length, width = q_ref.shape
    dim = width // heads
    scale = dim ** (-0.5)
    slots = n * cap
    local = plane * cap
    me = lax.axis_index("st")
    side = lax.axis_index("tp")
    z = me // plane
    p = me % plane
    base = z * local

    def remote(src, dst, send, recv, where):
        return pltpu.make_async_remote_copy(
            src_ref=src, dst_ref=dst, send_sem=send, recv_sem=recv, device_id=where, device_id_type=MESH
        )

    barrier = pltpu.get_barrier_semaphore()

    def greet(d, carry):
        pl.semaphore_signal(barrier, inc=1, device_id={"st": lax.rem(me + d, n)}, device_id_type=MESH)
        return carry

    lax.fori_loop(1, n, greet, 0)
    for d in range(1, parts):
        pl.semaphore_signal(barrier, inc=1, device_id={"tp": lax.rem(side + d, parts)}, device_id_type=MESH)
    pl.semaphore_wait(barrier, n - 1 + parts - 1)

    def mate(j):
        return {"st": z * plane + lax.rem(p + j, plane)}

    def back_mate(j):
        return {"st": z * plane + lax.rem(p + plane - j, plane)}

    def tab_copy(d):
        return remote(tab_ref, tabs_v.at[me], tab_send.at[d], tab_recv.at[d], {"st": lax.rem(me + d, n)})

    def ring_copy(s):
        src = q_ref if s == 0 else qcol[s - 1]
        where = {"st": lax.rem(z + 1, columns) * plane + p}
        return remote(src, qcol[s], ring_send.at[s], ring_recv.at[s], where)

    def query_copy(s, j):
        return remote(qout.at[s, j], qin.at[s, j], qs.at[s, j], qr.at[s, j], mate(j))

    def result_copies(s, j):
        mine = pl.ds(p * cap, cap)
        return (
            remote(rout.at[s, j], rin[s].at[mine], rs.at[s, j], rr.at[s, j], back_mate(j)),
            remote(lout.at[s, j], lin[s].at[mine], ls.at[s, j], lr.at[s, j], back_mate(j)),
        )

    def merged_copies(s):
        where = {"st": lax.rem(z + columns - s, columns) * plane + p}
        return (
            remote(mout.at[s - 1], mid.at[s - 1], ms.at[s - 1], mr.at[s - 1], where),
            remote(mlout.at[s - 1], mlin.at[s - 1], mls.at[s - 1], mlr.at[s - 1], where),
        )

    def look(s, j, i):
        row = lax.rem(z + columns - s, columns) * plane + lax.rem(p + plane - j, plane)
        return tabs_s[row, 0, i]

    def each(count, f, first=1):
        def body(i, carry):
            f(i)
            return carry

        lax.fori_loop(first, count, body, 0)

    each(n, lambda d: tab_copy(d).start())
    if columns > 1:
        ring_copy(0).start()
    own_copy = pltpu.make_async_copy(tab_ref, tabs_v.at[me], loc.at[0])
    own_copy.start()

    def select(s):
        block = q_ref if s == 0 else qcol[s - 1]

        def pick(j):
            o = z * plane + lax.rem(p + j, plane)
            for c in range(cap):
                i = slots + o * cap + c
                span = own_tab[i] if s == 0 else look(s, 0, i)
                qout[s, j, c] = block[span]

        each(plane, pick)
        each(plane, lambda j: query_copy(s, j).start())

    select(0)
    own_copy.wait()
    each(n, lambda d: tab_copy(d).wait_recv())
    to_smem = pltpu.make_async_copy(tabs_v, tabs_s, loc.at[1])
    to_smem.start()
    to_smem.wait()

    def attend(queries, passages, put):
        for c in range(cap):
            s_scr[c] = (
                lax.dot_general(
                    k_ref[passages[c]],
                    stacked_queries(queries[c], heads),
                    (((1,), (1,)), ((), ())),
                    preferred_element_type=f32,
                )
                * scale
            )
        totals = []
        levels = []
        for c in range(cap):
            s = s_scr[c]
            peak = jnp.max(s, axis=0, keepdims=True)
            w = jnp.exp(s - peak)
            total = jnp.sum(w, axis=0, keepdims=True)
            w_scr[c] = w.astype(bf16)
            totals.append(total)
            levels.append(peak + jnp.log(total))
        for c in range(cap):
            o = jnp.dot(vt_ref[passages[c]], w_scr[c], preferred_element_type=f32)
            put(c, (own_head(o, heads) / totals[c]).astype(bf16), levels[c])

    def attention(s):
        block = q_ref if s == 0 else qcol[s - 1]
        mine = me * cap
        spans_here = [look(s, 0, slots + mine + c) for c in range(cap)]
        passages = [look(s, 0, mine + c) for c in range(cap)]

        def put_here(c, value, level):
            rin[s][p * cap + c] = value
            lin[s][p * cap + c] = level

        attend([block[i] for i in spans_here], passages, put_here)

        def for_mate(j):
            query_copy(s, j).wait_recv()

            def put(c, value, level):
                rout[s, j, c] = value
                lout[s, j, c] = level

            attend([qin[s, j, c] for c in range(cap)], [look(s, j, mine + c) for c in range(cap)], put)

            @pl.when(j > 1)
            def _():
                for copy in result_copies(s, j - 1):
                    copy.start()

        each(plane, for_mate)
        if plane > 1:
            for copy in result_copies(s, plane - 1):
                copy.start()

    def gathered(s, span):
        levels, values = [], []
        for k in range(picks):
            i = look(s, 0, 2 * slots + span * picks + k) - base
            inside = (i >= 0) & (i < local)
            i = jnp.clip(i, 0, local - 1)
            levels.append(jnp.where(inside, lin[s][i], far))
            values.append(rin[s][i])
        return levels, values

    def weighted(levels, values):
        top = functools.reduce(jnp.maximum, levels)
        ws = [jnp.exp(level - top) for level in levels]
        total = sum(ws)
        summed = sum(w * value.astype(f32) for w, value in zip(ws, values))
        return summed / total, top + jnp.log(total)

    def wait_results(s):
        def one(j):
            for copy in result_copies(s, j):
                copy.wait_recv()

        each(plane, one)

    def merge(s):
        wait_results(s)

        def one(span):
            value, level = weighted(*gathered(s, span))
            mout[s - 1, span] = value.astype(bf16)
            mlout[s - 1, span] = level

        each(spans, one, 0)
        for copy in merged_copies(s):
            copy.start()

    for s in range(1, columns):
        ring_copy(s - 1).wait_recv()
        if s < columns - 1:
            ring_copy(s).start()
        select(s)
        if s > 1:
            attention(s - 1)
    if columns > 1:
        attention(columns - 1)
    for s in range(1, columns - 1):
        merge(s)
    attention(0)
    if columns > 1:
        merge(columns - 1)
    wait_results(0)
    for s in range(1, columns):
        for copy in merged_copies(s):
            copy.wait_recv()

    share = spans // parts
    rows = share * length

    def final(first, to):
        def one(i):
            span = first + i
            levels, values = gathered(0, span)
            for s in range(1, columns):
                levels.append(mlin[s - 1, span])
                values.append(mid[s - 1, span])
            memory, _ = weighted(levels, values)
            memory = memory.T
            memory = jnp.concatenate([memory[h * length : (h + 1) * length] for h in range(heads)], axis=1)
            at = pl.ds(pl.multiple_of(span * length, length), length)
            to(i, (gated_ref[at] + blend_ref[at] * memory).astype(bf16))

        each(share, one, 0)

    lanes = pl.ds(pl.multiple_of(side * width, width), width)

    def half_copy(d):
        return remote(half.at[d - 1], out_ref.at[:, lanes], ts.at[d - 1], tr.at[d - 1], {"tp": lax.rem(side + d, parts)})

    for d in range(1, parts):

        def keep(i, value):
            half[d - 1, pl.ds(pl.multiple_of(i * length, length), length)] = value

        final(lax.rem(side + d, parts) * share, keep)
        half_copy(d).start()

    def keep_own(i, value):
        out_ref[pl.ds(pl.multiple_of(i * length, length), length), lanes] = value

    final(side * share, keep_own)

    for d in range(1, parts):
        half_copy(d).wait()
    each(n, lambda d: tab_copy(d).wait_send())
    for s in range(columns - 1):
        ring_copy(s).wait_send()
    for s in range(columns):

        def done(j):
            query_copy(s, j).wait_send()
            for copy in result_copies(s, j):
                copy.wait_send()

        each(plane, done)
    for s in range(1, columns):
        for copy in merged_copies(s):
            copy.wait_send()


def per_device(
    tokens,
    route_ids,
    store,
    token_gain,
    store_gain,
    carry_weight,
    spatial_weight,
    spatial_gain,
    position_mix,
    position_bias,
    query_weight,
    key_weight,
    read_weight,
    blend_weight,
    output_weight,
):
    row_count, model = tokens.shape
    local_heads, block_length = position_mix.shape[:2]
    width = carry_weight.shape[1]
    head_dim = width // local_heads
    span_count, pick_count = route_ids.shape
    span_length = row_count // span_count
    store_count, passage_length = store.shape[:2]
    owner_count = lax.axis_size("st")
    requests = span_count * pick_count
    cap = max(1, 2 * requests // owner_count)
    slots = owner_count * cap

    flat_ids = route_ids.reshape(requests)
    owner = flat_ids // store_count
    order = jnp.arange(requests, dtype=jnp.int32)
    earlier = (owner[:, None] == owner[None, :]) & (order[None, :] < order[:, None])
    position = owner * cap + jnp.sum(earlier.astype(jnp.int32), axis=1)
    hit = position[None, :] == jnp.arange(slots, dtype=jnp.int32)[:, None]
    slot_local = jnp.sum(jnp.where(hit, (flat_ids % store_count)[None, :], 0), axis=1)
    slot_span = jnp.sum(jnp.where(hit, (order // pick_count)[None, :], 0), axis=1)
    table = jnp.concatenate([slot_local, slot_span, position])
    table = jnp.pad(table, (0, -table.shape[0] % 128))

    tile = 2 * span_length
    normed, queries = pl.pallas_call(
        functools.partial(query_kernel, span_length),
        grid=(row_count // tile,),
        in_specs=[
            pl.BlockSpec((tile, model), lambda i: (i, 0)),
            pl.BlockSpec((1, model), lambda i: (0, 0)),
            pl.BlockSpec((model, width), lambda i: (0, 0)),
        ],
        out_specs=[
            pl.BlockSpec((tile, model), lambda i: (i, 0)),
            pl.BlockSpec((tile // span_length, span_length, width), lambda i: (i, 0, 0)),
        ],
        out_shape=[
            jax.ShapeDtypeStruct((row_count, model), bf16),
            jax.ShapeDtypeStruct((span_count, span_length, width), bf16),
        ],
        cost_estimate=pl.CostEstimate(
            flops=2 * row_count * model * width, bytes_accessed=4 * row_count * model, transcendentals=0
        ),
        name="query",
    )(tokens, token_gain.reshape(1, model), query_weight)

    group = 2
    keys, values_t = pl.pallas_call(
        store_kernel,
        grid=(store_count // group,),
        in_specs=[
            pl.BlockSpec((group, passage_length, model), lambda i: (i, 0, 0)),
            pl.BlockSpec((1, model), lambda i: (0, 0)),
            pl.BlockSpec((model, width), lambda i: (0, 0)),
            pl.BlockSpec((model, width), lambda i: (0, 0)),
        ],
        out_specs=[
            pl.BlockSpec((group, passage_length, width), lambda i: (i, 0, 0)),
            pl.BlockSpec((group, width, passage_length), lambda i: (i, 0, 0)),
        ],
        out_shape=[
            jax.ShapeDtypeStruct((store_count, passage_length, width), bf16),
            jax.ShapeDtypeStruct((store_count, width, passage_length), bf16),
        ],
        cost_estimate=pl.CostEstimate(
            flops=4 * store_count * passage_length * model * width,
            bytes_accessed=2 * store_count * passage_length * model,
            transcendentals=0,
        ),
        name="store",
    )(store, store_gain.reshape(1, model), key_weight, read_weight)

    carry_branch = jnp.dot(normed, carry_weight, preferred_element_type=f32)
    spatial = jax.nn.gelu(jnp.dot(normed, spatial_weight, preferred_element_type=f32), approximate=False)
    total_width = width * lax.axis_size("tp")
    moment_one, moment_two = lax.psum(
        (jnp.sum(spatial, axis=1), jnp.sum(spatial * spatial, axis=1)), "tp"
    )
    channel_mean = (moment_one / total_width)[:, None]
    channel_spread = (moment_two / total_width)[:, None] - channel_mean * channel_mean
    spatial_in = (
        (spatial - channel_mean) * lax.rsqrt(channel_spread + norm_eps) * spatial_gain
    ).astype(bf16)
    blocks = spatial_in.reshape(row_count // block_length, block_length, local_heads, head_dim)
    mixed_blocks = jnp.einsum("hij,njhc->nihc", position_mix, blocks, preferred_element_type=f32)
    mixed_blocks = mixed_blocks + position_bias.T[None, :, :, None]
    gated_mix = jax.nn.gelu(carry_branch, approximate=False) * mixed_blocks.reshape(row_count, width)
    blend_gate = jax.nn.sigmoid(jnp.dot(normed, blend_weight, preferred_element_type=f32))

    parts = lax.axis_size("tp")
    columns = 4 if owner_count % 4 == 0 else 1
    plane = owner_count // columns
    local = plane * cap
    wide = local_heads * span_length
    vmem = pl.BlockSpec(memory_space=pltpu.VMEM)
    smem = pl.BlockSpec(memory_space=pltpu.SMEM)
    dma = pltpu.SemaphoreType.DMA
    by_rows = pl.pallas_call(
        functools.partial(route_kernel, (columns, plane, parts, local_heads, cap, pick_count)),
        in_specs=[smem] + [vmem] * 6,
        out_specs=vmem,
        out_shape=jax.ShapeDtypeStruct((row_count // parts, parts * width), bf16),
        scratch_shapes=[
            pltpu.VMEM((owner_count, 1, table.shape[0]), jnp.int32),
            pltpu.SMEM((owner_count, 1, table.shape[0]), jnp.int32),
            [pltpu.VMEM((span_count, span_length, width), bf16)] * columns,
            pltpu.VMEM((columns, plane, cap, span_length, width), bf16),
            pltpu.VMEM((columns, plane, cap, span_length, width), bf16),
            pltpu.VMEM((columns, plane, cap, head_dim, wide), bf16),
            pltpu.VMEM((columns, plane, cap, 1, wide), f32),
            [pltpu.VMEM((local, head_dim, wide), bf16)] * columns,
            [pltpu.VMEM((local, 1, wide), f32)] * columns,
            pltpu.VMEM((columns, span_count, head_dim, wide), bf16),
            pltpu.VMEM((columns, span_count, 1, wide), f32),
            pltpu.VMEM((columns, span_count, head_dim, wide), bf16),
            pltpu.VMEM((columns, span_count, 1, wide), f32),
            pltpu.VMEM((parts, row_count // parts, width), bf16),
            pltpu.VMEM((cap, passage_length, wide), f32),
            pltpu.VMEM((cap, passage_length, wide), bf16),
            dma((owner_count,)),
            dma((owner_count,)),
            dma((2,)),
            dma((columns,)),
            dma((columns,)),
            dma((columns, plane)),
            dma((columns, plane)),
            dma((columns, plane)),
            dma((columns, plane)),
            dma((columns, plane)),
            dma((columns, plane)),
            dma((columns,)),
            dma((columns,)),
            dma((columns,)),
            dma((columns,)),
            dma((parts,)),
            dma((parts,)),
        ],
        compiler_params=pltpu.CompilerParams(
            collective_id=0, has_side_effects=True, vmem_limit_bytes=48 * 2**20
        ),
        name="route",
    )(table, table.reshape(1, table.shape[0]), queries, keys, values_t, gated_mix, blend_gate)
    return jnp.dot(by_rows, output_weight, preferred_element_type=f32).astype(bf16)


def solution(mesh):
    in_specs = (
        P("st", None),
        P("st", None),
        P("st", None, None),
        P(),
        P(),
        P(None, "tp"),
        P(None, "tp"),
        P("tp"),
        P("tp", None, None),
        P("tp", None),
        P(None, "tp"),
        P(None, "tp"),
        P(None, "tp"),
        P(None, "tp"),
        P(),
    )
    out_specs = P(("st", "tp"), None)
    return jax.shard_map(
        per_device, mesh=mesh, in_specs=in_specs, out_specs=out_specs, check_vma=False
    )
```

```python
import functools

import jax
import jax.numpy as jnp
from jax import lax
from jax.experimental import pallas as pl
from jax.experimental.pallas import tpu as pltpu
from jax.sharding import PartitionSpec as P

norm_eps = 1e-06
bf16 = jnp.bfloat16
f32 = jnp.float32


def normed_rows(matrix, gain):
    values = matrix.astype(f32)
    scaled = values * lax.rsqrt(jnp.mean(values * values, axis=-1, keepdims=True) + norm_eps)
    return (scaled * gain).astype(bf16)

far = -1e30
MESH = pl.DeviceIdType.MESH


def stacked_queries(q, heads):
    length, width = q.shape
    dim = width // heads
    row_head = lax.broadcasted_iota(jnp.int32, (heads * length, width), 0) // length
    lane_head = lax.broadcasted_iota(jnp.int32, (heads * length, width), 1) // dim
    return jnp.where(row_head == lane_head, jnp.concatenate([q] * heads, axis=0), jnp.zeros((), bf16))


def own_head(o, heads):
    width, columns = o.shape
    dim, length = width // heads, columns // heads
    col_head = lax.broadcasted_iota(jnp.int32, (dim, columns), 1) // length
    out = o[0:dim]
    for h in range(1, heads):
        out = jnp.where(col_head == h, o[h * dim : (h + 1) * dim], out)
    return out


def erf_gelu(x):
    return 0.5 * x * (1.0 + lax.erf(x * 0.5**0.5))


def layer_kernel(
    sizes,
    own_tab,
    tab_ref,
    token_gain,
    store_gain,
    spatial_gain,
    bias_ref,
    mix_ref,
    tokens,
    store,
    wq,
    ws,
    wk,
    wv,
    wc,
    wb,
    out_ref,
    v,
):
    columns, plane, parts, heads, cap, picks, halves = sizes
    q_own, qcol, qout, qin = v["q_own"], v["qcol"], v["qout"], v["qin"]
    rout, lout, rin, lin = v["rout"], v["lout"], v["rin"], v["lin"]
    mout, mlout, mid, mlin, half = v["mout"], v["mlout"], v["mid"], v["mlin"], v["half"]
    tabs_v, tabs_s, normed = v["tabs_v"], v["tabs_s"], v["normed"]
    keys, values_t, w_ref = v["keys"], v["values_t"], v["w"]
    n = columns * plane
    spans, length, width = q_own.shape
    tiles, tile, model = normed.shape
    per = tile // length
    store_count = keys.shape[0]
    dim = width // heads
    scale = dim ** (-0.5)
    slots = n * cap
    local = plane * cap
    me = lax.axis_index("st")
    side = lax.axis_index("tp")
    z = me // plane
    p = me % plane
    base = z * local

    def each(count, f, first=0):
        def body(i, carry):
            f(i)
            return carry

        lax.fori_loop(first, count, body, 0)

    def remote(src, dst, send, recv, where):
        return pltpu.make_async_remote_copy(
            src_ref=src, dst_ref=dst, send_sem=send, recv_sem=recv, device_id=where, device_id_type=MESH
        )

    def token_copy(i):
        rows = pl.ds(pl.multiple_of(i * tile, tile), tile)
        return pltpu.make_async_copy(tokens.at[rows], v["tok"].at[i], v["tok_sem"].at[i])

    def store_copy(i):
        return pltpu.make_async_copy(store.at[i], v["st"].at[i], v["st_sem"].at[i])

    def weight_copy(i):
        return pltpu.make_async_copy((wq, ws, wk, wv, wc, wb)[i], w_ref.at[i], v["w_sem"].at[i])

    def mate(j):
        return {"st": z * plane + lax.rem(p + j, plane)}

    def back_mate(j):
        return {"st": z * plane + lax.rem(p + plane - j, plane)}

    def other(d):
        return {"tp": lax.rem(side + d, parts)}

    def tab_copy(d):
        return remote(tab_ref, tabs_v.at[me], v["tab_send"].at[d], v["tab_recv"].at[d], {"st": lax.rem(me + d, n)})

    def block(s):
        return q_own if s == 0 else qcol[s - 1]

    def ring_copy(s, h):
        piece = pl.ds(h * (spans // halves), spans // halves)
        where = {"st": lax.rem(z + 1, columns) * plane + p}
        send, recv = v["ring_send"].at[s, h], v["ring_recv"].at[s, h]
        return remote(block(s).at[piece], qcol[s].at[piece], send, recv, where)

    def query_copy(s, j):
        return remote(qout.at[s, j], qin.at[s, j], v["qs"].at[s, j], v["qr"].at[s, j], mate(j))

    def result_copies(s, j):
        mine = pl.ds(p * cap, cap)
        return (
            remote(rout.at[s, j], rin[s].at[mine], v["rs"].at[s, j], v["rr"].at[s, j], back_mate(j)),
            remote(lout.at[s, j], lin[s].at[mine], v["ls"].at[s, j], v["lr"].at[s, j], back_mate(j)),
        )

    def merged_copies(s):
        where = {"st": lax.rem(z + columns - s, columns) * plane + p}
        i = s - 1
        return (
            remote(mout.at[i], mid.at[i], v["ms"].at[i], v["mr"].at[i], where),
            remote(mlout.at[i], mlin.at[i], v["mls"].at[i], v["mlr"].at[i], where),
        )

    def moment_copy(d):
        return remote(v["mom"], v["mom_in"].at[d - 1], v["xs"].at[d - 1], v["xr"].at[d - 1], other(d))

    def look(s, j, i):
        row = lax.rem(z + columns - s, columns) * plane + lax.rem(p + plane - j, plane)
        return tabs_s[row, 0, i]

    weight_copy(0).start()
    each(tiles, lambda i: token_copy(i).start())
    for i in range(1, 6):
        weight_copy(i).start()
    each(store_count, lambda i: store_copy(i).start())

    barrier = pltpu.get_barrier_semaphore()

    def greet(d):
        pl.semaphore_signal(barrier, inc=1, device_id={"st": lax.rem(me + d, n)}, device_id_type=MESH)

    each(n, greet, 1)
    for d in range(1, parts):
        pl.semaphore_signal(barrier, inc=1, device_id=other(d), device_id_type=MESH)

    weight_copy(0).wait()

    def query(i):
        token_copy(i).wait()
        rows = normed_rows(v["tok"][i], token_gain[...])
        normed[i] = rows
        q = jnp.dot(rows, w_ref[0], preferred_element_type=f32).astype(bf16)
        for s in range(per):
            q_own[i * per + s] = q[s * length : (s + 1) * length]

    for h in range(halves):
        each(tiles * (h + 1) // halves, query, tiles * h // halves)
        if h == 0:
            pl.semaphore_wait(barrier, n - 1 + parts - 1)
        if columns > 1:
            ring_copy(0, h).start()
    each(n, lambda d: tab_copy(d).start(), 1)
    own_copy = pltpu.make_async_copy(tab_ref, tabs_v.at[me], v["loc"].at[0])
    own_copy.start()

    def select(s):
        def pick(j):
            o = z * plane + lax.rem(p + j, plane)
            for c in range(cap):
                i = slots + o * cap + c
                span = own_tab[i] if s == 0 else look(s, 0, i)
                qout[s, j, c] = block(s)[span]

        each(plane, pick, 1)
        each(plane, lambda j: query_copy(s, j).start(), 1)

    select(0)

    def spatial_first(i):
        x = jnp.dot(normed[i], w_ref[1], preferred_element_type=f32)
        x = erf_gelu(x)
        v["spatial"][i] = x
        one = jnp.sum(x, axis=1, keepdims=True)
        two = jnp.sum(x * x, axis=1, keepdims=True)
        lane = lax.broadcasted_iota(jnp.int32, (tile, 128), 1)
        v["mom"][i] = jnp.where(lane < 64, one, two)

    weight_copy(1).wait()
    each(tiles, spatial_first)
    for d in range(1, parts):
        moment_copy(d).start()

    def project(i):
        store_copy(i).wait()
        rows = normed_rows(v["st"][i], store_gain[...])
        keys[i] = jnp.dot(rows, w_ref[2], preferred_element_type=f32).astype(bf16)
        values_t[i] = jnp.dot(rows, w_ref[3], preferred_element_type=f32).T.astype(bf16)

    def spatial_rest():
        for d in range(1, parts):
            moment_copy(d).wait_recv()
        weight_copy(4).wait()
        weight_copy(5).wait()

        def one(i):
            mom = v["mom"][i]
            for d in range(1, parts):
                mom = mom + v["mom_in"][d - 1, i]
            mom = mom / (width * parts)
            mean = mom[:, 0:1]
            spread = mom[:, 64:65] - mean * mean
            x = (v["spatial"][i] - mean) * lax.rsqrt(spread + norm_eps) * spatial_gain[...]
            x = x.astype(bf16)
            mixed = [
                jnp.dot(mix_ref[h], x[:, h * dim : (h + 1) * dim], preferred_element_type=f32)
                + bias_ref[:, h : h + 1]
                for h in range(heads)
            ]
            mixed = jnp.concatenate(mixed, axis=1)
            carry = jnp.dot(normed[i], w_ref[4], preferred_element_type=f32)
            v["gated"][i] = erf_gelu(carry) * mixed
            v["blend"][i] = jax.nn.sigmoid(jnp.dot(normed[i], w_ref[5], preferred_element_type=f32))

        each(tiles, one)

    def attend(queries, passages, put):
        for c in range(cap):
            v["s"][c] = (
                lax.dot_general(
                    keys[passages[c]],
                    stacked_queries(queries[c], heads),
                    (((1,), (1,)), ((), ())),
                    preferred_element_type=f32,
                )
                * scale
            )
        totals = []
        levels = []
        for c in range(cap):
            s = v["s"][c]
            peak = jnp.max(s, axis=0, keepdims=True)
            w = jnp.exp(s - peak)
            total = jnp.sum(w, axis=0, keepdims=True)
            v["p"][c] = w.astype(bf16)
            totals.append(total)
            levels.append(peak + jnp.log(total))
        for c in range(cap):
            o = jnp.dot(values_t[passages[c]], v["p"][c], preferred_element_type=f32)
            put(c, (own_head(o, heads) / totals[c]).astype(bf16), levels[c])

    def send_results(s, j):
        for copy in result_copies(s, j):
            copy.start()

    def attention(s, send=True):
        mine = me * cap

        def for_mate(j):
            query_copy(s, j).wait_recv()

            def put(c, value, level):
                rout[s, j, c] = value
                lout[s, j, c] = level

            attend([qin[s, j, c] for c in range(cap)], [look(s, j, mine + c) for c in range(cap)], put)
            if send:

                @pl.when(j > 1)
                def _():
                    send_results(s, j - 1)

        each(plane, for_mate, 1)

        def put_here(c, value, level):
            rin[s][p * cap + c] = value
            lin[s][p * cap + c] = level

        here = [block(s)[look(s, 0, slots + mine + c)] for c in range(cap)]
        if send and plane > 1:
            send_results(s, plane - 1)
        attend(here, [look(s, 0, mine + c) for c in range(cap)], put_here)

    def source(s, span, k):
        i = look(s, 0, 2 * slots + span * picks + k) - base
        return jnp.clip(i, 0, local - 1), (i >= 0) & (i < local)

    def weigh(s, more):
        def one(span):
            for k in range(picks):
                i, inside = source(s, span, k)
                v["lev"][k, pl.ds(span, 1)] = jnp.where(inside, lin[s][i], far)

        each(spans, one)
        levels = [v["lev"][k] for k in range(picks)] + more
        top = functools.reduce(jnp.maximum, levels)
        ws = [jnp.exp(level - top) for level in levels]
        total = sum(ws)
        for k, w in enumerate(ws):
            v["wt"][k] = w / total
        return top + jnp.log(total)

    def summed(s, span, more):
        at = pl.ds(span, 1)
        terms = [v["wt"][k, at] * rin[s][source(s, span, k)[0]].astype(f32) for k in range(picks)]
        for k, ref in enumerate(more):
            terms.append(v["wt"][picks + k, at] * ref[span].astype(f32))
        return sum(terms)

    def wait_results(s):
        def one(j):
            for copy in result_copies(s, j):
                copy.wait_recv()

        each(plane, one, 1)

    def merge(s):
        wait_results(s)
        mlout[s - 1] = weigh(s, [])

        def one(span):
            mout[s - 1, span] = summed(s, span, []).astype(bf16)

        each(spans, one)
        for copy in merged_copies(s):
            copy.start()

    own_copy.wait()
    weight_copy(2).wait()
    weight_copy(3).wait()
    steps = max(columns - 1, 1)
    cut = [store_count * min(i, 2) // 2 for i in range(steps + 1)] if steps > 1 else [0, store_count]
    for s in range(1, columns):
        each(cut[s], project, cut[s - 1])
        if s == 1:
            each(n, lambda d: tab_copy(d).wait_recv(), 1)
            to_smem = pltpu.make_async_copy(tabs_v, tabs_s, v["loc"].at[1])
            to_smem.start()
            to_smem.wait()
        for h in range(halves):
            ring_copy(s - 1, h).wait_recv()
            if s < columns - 1:
                ring_copy(s, h).start()
        select(s)
        if s > 1:
            attention(s - 1)
        if s == 2:
            spatial_rest()
    if columns > 1:
        attention(columns - 1)
    attention(0)
    for s in range(1, columns):
        merge(s)
    wait_results(0)
    for s in range(1, columns):
        for copy in merged_copies(s):
            copy.wait_recv()

    share = spans // parts
    weigh(0, [mlin[s - 1] for s in range(1, columns)])
    lanes = pl.ds(pl.multiple_of(side * width, width), width)

    def final(first, to):
        def one(i):
            span = first + i
            memory = summed(0, span, [mid.at[s - 1] for s in range(1, columns)]).T
            memory = jnp.concatenate([memory[h * length : (h + 1) * length] for h in range(heads)], axis=1)
            at = pl.ds(pl.multiple_of(lax.rem(span, per) * length, length), length)
            t = span // per
            to(i, (v["gated"][t, at] + v["blend"][t, at] * memory).astype(bf16))

        each(share, one)

    def half_copy(d):
        i = d - 1
        return remote(half.at[i], out_ref.at[:, lanes], v["ts"].at[i], v["tr"].at[i], other(d))

    def rows_of(i):
        return pl.ds(pl.multiple_of(i * length, length), length)

    for d in range(1, parts):

        def keep(i, value):
            half[d - 1, rows_of(i)] = value

        final(lax.rem(side + d, parts) * share, keep)
        half_copy(d).start()

    def keep_own(i, value):
        out_ref[rows_of(i), lanes] = value

    final(side * share, keep_own)

    for d in range(1, parts):
        half_copy(d).wait()
        moment_copy(d).wait_send()
    each(n, lambda d: tab_copy(d).wait_send(), 1)
    for s in range(columns - 1):
        for h in range(halves):
            ring_copy(s, h).wait_send()
    for s in range(columns):

        def done(j):
            query_copy(s, j).wait_send()
            for copy in result_copies(s, j):
                copy.wait_send()

        each(plane, done, 1)
    for s in range(1, columns):
        for copy in merged_copies(s):
            copy.wait_send()


def per_device(
    tokens,
    route_ids,
    store,
    token_gain,
    store_gain,
    carry_weight,
    spatial_weight,
    spatial_gain,
    position_mix,
    position_bias,
    query_weight,
    key_weight,
    read_weight,
    blend_weight,
    output_weight,
):
    row_count, model = tokens.shape
    local_heads, block_length = position_mix.shape[:2]
    width = carry_weight.shape[1]
    head_dim = width // local_heads
    span_count, pick_count = route_ids.shape
    span_length = row_count // span_count
    store_count, passage_length = store.shape[:2]
    owner_count = lax.axis_size("st")
    requests = span_count * pick_count
    cap = max(1, 2 * requests // owner_count)
    slots = owner_count * cap

    flat_ids = route_ids.reshape(requests)
    owner = flat_ids // store_count
    order = jnp.arange(requests, dtype=jnp.int32)
    earlier = (owner[:, None] == owner[None, :]) & (order[None, :] < order[:, None])
    position = owner * cap + jnp.sum(earlier.astype(jnp.int32), axis=1)
    hit = position[None, :] == jnp.arange(slots, dtype=jnp.int32)[:, None]
    slot_local = jnp.sum(jnp.where(hit, (flat_ids % store_count)[None, :], 0), axis=1)
    slot_span = jnp.sum(jnp.where(hit, (order // pick_count)[None, :], 0), axis=1)
    table = jnp.concatenate([slot_local, slot_span, position])
    table = jnp.pad(table, (0, -table.shape[0] % 128))

    parts = lax.axis_size("tp")
    columns = 4 if owner_count % 4 == 0 else 1
    plane = owner_count // columns
    local = plane * cap
    wide = local_heads * span_length
    tiles = row_count // block_length
    halves = 2 if tiles % 2 == 0 else 1
    tab_size = table.shape[0]
    vmem = pl.BlockSpec(memory_space=pltpu.VMEM)
    smem = pl.BlockSpec(memory_space=pltpu.SMEM)
    hbm = pl.BlockSpec(memory_space=pl.ANY)
    dma = pltpu.SemaphoreType.DMA
    V = pltpu.VMEM
    scratch = dict(
        tok=V((tiles, block_length, model), bf16),
        normed=V((tiles, block_length, model), bf16),
        st=V((store_count, passage_length, model), bf16),
        w=V((6, model, width), bf16),
        keys=V((store_count, passage_length, width), bf16),
        values_t=V((store_count, width, passage_length), bf16),
        spatial=V((tiles, block_length, width), f32),
        gated=V((tiles, block_length, width), f32),
        blend=V((tiles, block_length, width), f32),
        mom=V((tiles, block_length, 128), f32),
        mom_in=V((parts, tiles, block_length, 128), f32),
        tabs_v=V((owner_count, 1, tab_size), jnp.int32),
        tabs_s=pltpu.SMEM((owner_count, 1, tab_size), jnp.int32),
        q_own=V((span_count, span_length, width), bf16),
        qcol=[V((span_count, span_length, width), bf16)] * (columns - 1),
        qout=V((columns, plane, cap, span_length, width), bf16),
        qin=V((columns, plane, cap, span_length, width), bf16),
        rout=V((columns, plane, cap, head_dim, wide), bf16),
        lout=V((columns, plane, cap, 1, wide), f32),
        rin=[V((local, head_dim, wide), bf16)] * columns,
        lin=[V((local, 1, wide), f32)] * columns,
        mout=V((columns, span_count, head_dim, wide), bf16),
        mlout=V((columns, span_count, wide), f32),
        mid=V((columns, span_count, head_dim, wide), bf16),
        mlin=V((columns, span_count, wide), f32),
        lev=V((pick_count, span_count, wide), f32),
        wt=V((pick_count + columns, span_count, wide), f32),
        half=V((parts, row_count // parts, width), bf16),
        s=V((cap, passage_length, wide), f32),
        p=V((cap, passage_length, wide), bf16),
        tok_sem=dma((tiles,)),
        st_sem=dma((store_count,)),
        w_sem=dma((6,)),
        loc=dma((2,)),
        tab_send=dma((owner_count,)),
        tab_recv=dma((owner_count,)),
        ring_send=dma((columns, halves)),
        ring_recv=dma((columns, halves)),
        **{name: dma((columns, plane)) for name in ("qs", "qr", "rs", "rr", "ls", "lr")},
        **{name: dma((columns,)) for name in ("ms", "mr", "mls", "mlr")},
        **{name: dma((parts,)) for name in ("ts", "tr", "xs", "xr")},
    )
    by_rows = pl.pallas_call(
        functools.partial(layer_kernel, (columns, plane, parts, local_heads, cap, pick_count, halves)),
        in_specs=[smem] + [vmem] * 6 + [hbm] * 8,
        out_specs=vmem,
        out_shape=jax.ShapeDtypeStruct((row_count // parts, parts * width), bf16),
        scratch_shapes=[scratch],
        compiler_params=pltpu.CompilerParams(
            collective_id=0, has_side_effects=True, vmem_limit_bytes=60 * 2**20
        ),
        name="layer",
    )(
        table,
        table.reshape(1, tab_size),
        token_gain.reshape(1, model),
        store_gain.reshape(1, model),
        spatial_gain.reshape(1, width),
        position_bias.T,
        position_mix,
        tokens,
        store,
        query_weight,
        spatial_weight,
        key_weight,
        read_weight,
        carry_weight,
        blend_weight,
    )
    return jnp.dot(by_rows, output_weight, preferred_element_type=f32).astype(bf16)


def solution(mesh):
    in_specs = (
        P("st", None),
        P("st", None),
        P("st", None, None),
        P(),
        P(),
        P(None, "tp"),
        P(None, "tp"),
        P("tp"),
        P("tp", None, None),
        P("tp", None),
        P(None, "tp"),
        P(None, "tp"),
        P(None, "tp"),
        P(None, "tp"),
        P(),
    )
    out_specs = P(("st", "tp"), None)
    return jax.shard_map(
        per_device, mesh=mesh, in_specs=in_specs, out_specs=out_specs, check_vma=False
    )
```

```python
import functools

import jax
import jax.numpy as jnp
from jax import lax
from jax.experimental import pallas as pl
from jax.experimental.pallas import tpu as pltpu
from jax.sharding import PartitionSpec as P

norm_eps = 1e-06
bf16 = jnp.bfloat16
f32 = jnp.float32


def normed_rows(matrix, gain):
    values = matrix.astype(f32)
    scaled = values * lax.rsqrt(jnp.mean(values * values, axis=-1, keepdims=True) + norm_eps)
    return (scaled * gain).astype(bf16)

far = -1e30
MESH = pl.DeviceIdType.MESH


def stacked_queries(q, heads):
    length, width = q.shape
    dim = width // heads
    row_head = lax.broadcasted_iota(jnp.int32, (heads * length, width), 0) // length
    lane_head = lax.broadcasted_iota(jnp.int32, (heads * length, width), 1) // dim
    return jnp.where(row_head == lane_head, jnp.concatenate([q] * heads, axis=0), jnp.zeros((), bf16))


def own_head(o, heads):
    width, columns = o.shape
    dim, length = width // heads, columns // heads
    col_head = lax.broadcasted_iota(jnp.int32, (dim, columns), 1) // length
    out = o[0:dim]
    for h in range(1, heads):
        out = jnp.where(col_head == h, o[h * dim : (h + 1) * dim], out)
    return out


def erf_gelu(x):
    return 0.5 * x * (1.0 + lax.erf(x * 0.5**0.5))


def layer_kernel(
    sizes,
    own_tab,
    tab_ref,
    token_gain,
    store_gain,
    spatial_gain,
    bias_ref,
    mix_ref,
    tokens,
    store,
    wq,
    ws,
    wk,
    wv,
    wc,
    wb,
    out_ref,
    v,
):
    columns, plane, parts, heads, cap, picks, halves = sizes
    q_own, qcol, qout, qin = v["q_own"], v["qcol"], v["qout"], v["qin"]
    rout, lout, rin, lin = v["rout"], v["lout"], v["rin"], v["lin"]
    mout, mlout, mid, mlin, half = v["mout"], v["mlout"], v["mid"], v["mlin"], v["half"]
    tabs_v, tabs_s, normed = v["tabs_v"], v["tabs_s"], v["normed"]
    keys, values_t, w_ref = v["keys"], v["values_t"], v["w"]
    n = columns * plane
    spans, length, width = q_own.shape
    tiles, tile, model = normed.shape
    per = tile // length
    store_count = keys.shape[0]
    dim = width // heads
    scale = dim ** (-0.5)
    slots = n * cap
    local = plane * cap
    me = lax.axis_index("st")
    side = lax.axis_index("tp")
    z = me // plane
    p = me % plane
    base = z * local
    following = {"st": lax.rem(z + 1, columns) * plane + p}
    group = spans // halves

    def each(count, f, first=0):
        def body(i, carry):
            f(i)
            return carry

        lax.fori_loop(first, count, body, 0)

    def remote(src, dst, send, recv, where):
        return pltpu.make_async_remote_copy(
            src_ref=src, dst_ref=dst, send_sem=send, recv_sem=recv, device_id=where, device_id_type=MESH
        )

    def token_copy(i):
        rows = pl.ds(pl.multiple_of(i * tile, tile), tile)
        return pltpu.make_async_copy(tokens.at[rows], v["tok"].at[i], v["tok_sem"].at[i])

    def store_copy(i):
        return pltpu.make_async_copy(store.at[i], v["st"].at[i], v["st_sem"].at[i])

    def weight_copy(i):
        return pltpu.make_async_copy((wq, ws, wk, wv, wc, wb)[i], w_ref.at[i], v["w_sem"].at[i])

    def mate(j):
        return {"st": z * plane + lax.rem(p + j, plane)}

    def back_mate(j):
        return {"st": z * plane + lax.rem(p + plane - j, plane)}

    def other(d):
        return {"tp": lax.rem(side + d, parts)}

    def tab_copy(d):
        return remote(tab_ref, tabs_v.at[me], v["tab_send"].at[d], v["tab_recv"].at[d], {"st": lax.rem(me + d, n)})

    def block(s):
        return q_own if s == 0 else qcol[s - 1]

    def ring_copy(s, h):
        piece = pl.ds(h * (spans // halves), spans // halves)
        send, recv = v["ring_send"].at[s, h], v["ring_recv"].at[s, h]
        return remote(block(s).at[piece], qcol[s].at[piece], send, recv, following)

    def query_copy(s, j):
        return remote(qout.at[s, j], qin.at[s, j], v["qs"].at[s, j], v["qr"].at[s, j], mate(j))

    def result_copies(s, j):
        mine = pl.ds(p * cap, cap)
        return (
            remote(rout.at[s, j], rin[s].at[mine], v["rs"].at[s, j], v["rr"].at[s, j], back_mate(j)),
            remote(lout.at[s, j], lin[s].at[mine], v["ls"].at[s, j], v["lr"].at[s, j], back_mate(j)),
        )

    def merged_copies(s, h):
        i = s - 1
        return (
            remote(mout.at[i, h], mid.at[i, h], v["ms"].at[i, h], v["mr"].at[i, h], following),
            remote(mlout.at[i, h], mlin.at[i, h], v["mls"].at[i, h], v["mlr"].at[i, h], following),
        )

    def moment_copy(d):
        return remote(v["mom"], v["mom_in"].at[d - 1], v["xs"].at[d - 1], v["xr"].at[d - 1], other(d))

    def look(s, j, i):
        row = lax.rem(z + columns - s, columns) * plane + lax.rem(p + plane - j, plane)
        return tabs_s[row, 0, i]

    weight_copy(0).start()
    each(tiles, lambda i: token_copy(i).start())
    for i in range(1, 6):
        weight_copy(i).start()
    each(store_count, lambda i: store_copy(i).start())

    barrier = pltpu.get_barrier_semaphore()

    def greet(d):
        pl.semaphore_signal(barrier, inc=1, device_id={"st": lax.rem(me + d, n)}, device_id_type=MESH)

    each(n, greet, 1)
    for d in range(1, parts):
        pl.semaphore_signal(barrier, inc=1, device_id=other(d), device_id_type=MESH)

    weight_copy(0).wait()

    def query(i):
        token_copy(i).wait()
        rows = normed_rows(v["tok"][i], token_gain[...])
        normed[i] = rows
        q = jnp.dot(rows, w_ref[0], preferred_element_type=f32).astype(bf16)
        for s in range(per):
            q_own[i * per + s] = q[s * length : (s + 1) * length]

    for h in range(halves):
        each(tiles * (h + 1) // halves, query, tiles * h // halves)
        if h == 0:
            pl.semaphore_wait(barrier, n - 1 + parts - 1)
        if columns > 1:
            ring_copy(0, h).start()
    each(n, lambda d: tab_copy(d).start(), 1)
    own_copy = pltpu.make_async_copy(tab_ref, tabs_v.at[me], v["loc"].at[0])
    own_copy.start()

    def select(s):
        def pick(j):
            o = z * plane + lax.rem(p + j, plane)
            for c in range(cap):
                i = slots + o * cap + c
                span = own_tab[i] if s == 0 else look(s, 0, i)
                qout[s, j, c] = block(s)[span]

        each(plane, pick, 1)
        each(plane, lambda j: query_copy(s, j).start(), 1)

    select(0)

    def spatial_first(i):
        x = jnp.dot(normed[i], w_ref[1], preferred_element_type=f32)
        x = erf_gelu(x)
        v["spatial"][i] = x
        one = jnp.sum(x, axis=1, keepdims=True)
        two = jnp.sum(x * x, axis=1, keepdims=True)
        lane = lax.broadcasted_iota(jnp.int32, (tile, 128), 1)
        v["mom"][i] = jnp.where(lane < 64, one, two)

    weight_copy(1).wait()
    each(tiles, spatial_first)
    for d in range(1, parts):
        moment_copy(d).start()

    def project(i):
        store_copy(i).wait()
        rows = normed_rows(v["st"][i], store_gain[...])
        keys[i] = jnp.dot(rows, w_ref[2], preferred_element_type=f32).astype(bf16)
        values_t[i] = jnp.dot(rows, w_ref[3], preferred_element_type=f32).T.astype(bf16)

    def spatial_rest():
        for d in range(1, parts):
            moment_copy(d).wait_recv()
        weight_copy(4).wait()
        weight_copy(5).wait()

        def one(i):
            mom = v["mom"][i]
            for d in range(1, parts):
                mom = mom + v["mom_in"][d - 1, i]
            mom = mom / (width * parts)
            mean = mom[:, 0:1]
            spread = mom[:, 64:65] - mean * mean
            x = (v["spatial"][i] - mean) * lax.rsqrt(spread + norm_eps) * spatial_gain[...]
            x = x.astype(bf16)
            mixed = [
                jnp.dot(mix_ref[h], x[:, h * dim : (h + 1) * dim], preferred_element_type=f32)
                + bias_ref[:, h : h + 1]
                for h in range(heads)
            ]
            mixed = jnp.concatenate(mixed, axis=1)
            carry = jnp.dot(normed[i], w_ref[4], preferred_element_type=f32)
            v["gated"][i] = erf_gelu(carry) * mixed
            v["blend"][i] = jax.nn.sigmoid(jnp.dot(normed[i], w_ref[5], preferred_element_type=f32))

        each(tiles, one)

    def attend(queries, passages, put):
        for c in range(cap):
            v["s"][c] = (
                lax.dot_general(
                    keys[passages[c]],
                    stacked_queries(queries[c], heads),
                    (((1,), (1,)), ((), ())),
                    preferred_element_type=f32,
                )
                * scale
            )
        totals = []
        levels = []
        for c in range(cap):
            s = v["s"][c]
            peak = jnp.max(s, axis=0, keepdims=True)
            w = jnp.exp(s - peak)
            total = jnp.sum(w, axis=0, keepdims=True)
            v["p"][c] = w.astype(bf16)
            totals.append(total)
            levels.append(peak + jnp.log(total))
        for c in range(cap):
            o = jnp.dot(values_t[passages[c]], v["p"][c], preferred_element_type=f32)
            put(c, (own_head(o, heads) / totals[c]).astype(bf16), levels[c])

    def send_results(s, j):
        for copy in result_copies(s, j):
            copy.start()

    def attention(s, send=True):
        mine = me * cap

        def for_mate(j):
            query_copy(s, j).wait_recv()

            def put(c, value, level):
                rout[s, j, c] = value
                lout[s, j, c] = level

            attend([qin[s, j, c] for c in range(cap)], [look(s, j, mine + c) for c in range(cap)], put)
            if send:

                @pl.when(j > 1)
                def _():
                    send_results(s, j - 1)

        each(plane, for_mate, 1)

        def put_here(c, value, level):
            rin[s][p * cap + c] = value
            lin[s][p * cap + c] = level

        here = [block(s)[look(s, 0, slots + mine + c)] for c in range(cap)]
        if send and plane > 1:
            send_results(s, plane - 1)
        attend(here, [look(s, 0, mine + c) for c in range(cap)], put_here)

    def source(s, span, k):
        i = look(s, 0, 2 * slots + span * picks + k) - base
        return jnp.clip(i, 0, local - 1), (i >= 0) & (i < local)

    def weigh(s, h, more):
        def one(i):
            for k in range(picks):
                at, inside = source(s, h * group + i, k)
                v["lev"][k, pl.ds(i, 1)] = jnp.where(inside, lin[s][at], far)

        each(group, one)
        levels = [v["lev"][k] for k in range(picks)] + more
        top = functools.reduce(jnp.maximum, levels)
        ws = [jnp.exp(level - top) for level in levels]
        total = sum(ws)
        for k, w in enumerate(ws):
            v["wt"][k] = w / total
        return top + jnp.log(total)

    def summed(s, h, i, more):
        at = pl.ds(i, 1)
        terms = [v["wt"][k, at] * rin[s][source(s, h * group + i, k)[0]].astype(f32) for k in range(picks)]
        for k, ref in enumerate(more):
            terms.append(v["wt"][picks + k, at] * ref[i].astype(f32))
        return sum(terms)

    def wait_results(s):
        def one(j):
            for copy in result_copies(s, j):
                copy.wait_recv()

        each(plane, one, 1)

    def arrived(s, h):
        if (s if s else columns) < 2:
            return [], []
        i = (s if s else columns) - 2
        for copy in merged_copies(i + 1, h):
            copy.wait_recv()
        return [mlin[i, h]], [mid.at[i, h]]

    def merge(s):
        wait_results(s)
        for d in range(1, halves + 1):
            h = lax.rem(side + d, halves)
            levels, blocks = arrived(s, h)
            mlout[s - 1, h] = weigh(s, h, levels)

            def one(i):
                mout[s - 1, h, i] = summed(s, h, i, blocks).astype(bf16)

            each(group, one)
            for copy in merged_copies(s, h):
                copy.start()

    own_copy.wait()
    weight_copy(2).wait()
    weight_copy(3).wait()
    steps = max(columns - 1, 1)
    cut = [store_count * min(i, 2) // 2 for i in range(steps + 1)] if steps > 1 else [0, store_count]
    for s in range(1, columns):
        each(cut[s], project, cut[s - 1])
        if s == 1:
            each(n, lambda d: tab_copy(d).wait_recv(), 1)
            to_smem = pltpu.make_async_copy(tabs_v, tabs_s, v["loc"].at[1])
            to_smem.start()
            to_smem.wait()
        for h in range(halves):
            ring_copy(s - 1, h).wait_recv()
            if s < columns - 1:
                ring_copy(s, h).start()
        select(s)
        if s > 1:
            attention(s - 1)
        if s == 2:
            spatial_rest()
    for s in range(1, columns - 1):
        merge(s)
        if s == 1:
            attention(0, False)
            attention(columns - 1)
            each(plane, lambda j: send_results(0, j), 1)
    if columns > 1:
        merge(columns - 1)
    wait_results(0)

    lanes = pl.ds(pl.multiple_of(side * width, width), width)

    def final(h, to):
        levels, blocks = arrived(0, h)
        weigh(0, h, levels)

        def one(i):
            span = h * group + i
            memory = summed(0, h, i, blocks).T
            memory = jnp.concatenate([memory[c * length : (c + 1) * length] for c in range(heads)], axis=1)
            at = pl.ds(pl.multiple_of(lax.rem(span, per) * length, length), length)
            t = span // per
            to(i, (v["gated"][t, at] + v["blend"][t, at] * memory).astype(bf16))

        each(group, one)

    def half_copy(d):
        i = d - 1
        return remote(half.at[i], out_ref.at[:, lanes], v["ts"].at[i], v["tr"].at[i], other(d))

    def rows_of(i):
        return pl.ds(pl.multiple_of(i * length, length), length)

    for d in range(1, parts):

        def keep(i, value):
            half[d - 1, rows_of(i)] = value

        final(lax.rem(side + d, parts), keep)
        half_copy(d).start()

    def keep_own(i, value):
        out_ref[rows_of(i), lanes] = value

    final(side, keep_own)

    for d in range(1, parts):
        half_copy(d).wait()
        moment_copy(d).wait_send()
    each(n, lambda d: tab_copy(d).wait_send(), 1)
    for s in range(columns - 1):
        for h in range(halves):
            ring_copy(s, h).wait_send()
    for s in range(columns):

        def done(j):
            query_copy(s, j).wait_send()
            for copy in result_copies(s, j):
                copy.wait_send()

        each(plane, done, 1)
    for s in range(1, columns):
        for h in range(halves):
            for copy in merged_copies(s, h):
                copy.wait_send()


def per_device(
    tokens,
    route_ids,
    store,
    token_gain,
    store_gain,
    carry_weight,
    spatial_weight,
    spatial_gain,
    position_mix,
    position_bias,
    query_weight,
    key_weight,
    read_weight,
    blend_weight,
    output_weight,
):
    row_count, model = tokens.shape
    local_heads, block_length = position_mix.shape[:2]
    width = carry_weight.shape[1]
    head_dim = width // local_heads
    span_count, pick_count = route_ids.shape
    span_length = row_count // span_count
    store_count, passage_length = store.shape[:2]
    owner_count = lax.axis_size("st")
    requests = span_count * pick_count
    cap = max(1, 2 * requests // owner_count)
    slots = owner_count * cap

    flat_ids = route_ids.reshape(requests)
    owner = flat_ids // store_count
    order = jnp.arange(requests, dtype=jnp.int32)
    earlier = (owner[:, None] == owner[None, :]) & (order[None, :] < order[:, None])
    position = owner * cap + jnp.sum(earlier.astype(jnp.int32), axis=1)
    hit = position[None, :] == jnp.arange(slots, dtype=jnp.int32)[:, None]
    slot_local = jnp.sum(jnp.where(hit, (flat_ids % store_count)[None, :], 0), axis=1)
    slot_span = jnp.sum(jnp.where(hit, (order // pick_count)[None, :], 0), axis=1)
    table = jnp.concatenate([slot_local, slot_span, position])
    table = jnp.pad(table, (0, -table.shape[0] % 128))

    parts = lax.axis_size("tp")
    columns = 4 if owner_count % 4 == 0 else 1
    plane = owner_count // columns
    local = plane * cap
    wide = local_heads * span_length
    tiles = row_count // block_length
    halves = parts
    group = span_count // halves
    tab_size = table.shape[0]
    vmem = pl.BlockSpec(memory_space=pltpu.VMEM)
    smem = pl.BlockSpec(memory_space=pltpu.SMEM)
    hbm = pl.BlockSpec(memory_space=pl.ANY)
    dma = pltpu.SemaphoreType.DMA
    V = pltpu.VMEM
    scratch = dict(
        tok=V((tiles, block_length, model), bf16),
        normed=V((tiles, block_length, model), bf16),
        st=V((store_count, passage_length, model), bf16),
        w=V((6, model, width), bf16),
        keys=V((store_count, passage_length, width), bf16),
        values_t=V((store_count, width, passage_length), bf16),
        spatial=V((tiles, block_length, width), f32),
        gated=V((tiles, block_length, width), f32),
        blend=V((tiles, block_length, width), f32),
        mom=V((tiles, block_length, 128), f32),
        mom_in=V((parts, tiles, block_length, 128), f32),
        tabs_v=V((owner_count, 1, tab_size), jnp.int32),
        tabs_s=pltpu.SMEM((owner_count, 1, tab_size), jnp.int32),
        q_own=V((span_count, span_length, width), bf16),
        qcol=[V((span_count, span_length, width), bf16)] * (columns - 1),
        qout=V((columns, plane, cap, span_length, width), bf16),
        qin=V((columns, plane, cap, span_length, width), bf16),
        rout=V((columns, plane, cap, head_dim, wide), bf16),
        lout=V((columns, plane, cap, 1, wide), f32),
        rin=[V((local, head_dim, wide), bf16)] * columns,
        lin=[V((local, 1, wide), f32)] * columns,
        mout=V((columns, halves, group, head_dim, wide), bf16),
        mlout=V((columns, halves, group, wide), f32),
        mid=V((columns, halves, group, head_dim, wide), bf16),
        mlin=V((columns, halves, group, wide), f32),
        lev=V((pick_count, group, wide), f32),
        wt=V((pick_count + 1, group, wide), f32),
        half=V((parts, row_count // parts, width), bf16),
        s=V((cap, passage_length, wide), f32),
        p=V((cap, passage_length, wide), bf16),
        tok_sem=dma((tiles,)),
        st_sem=dma((store_count,)),
        w_sem=dma((6,)),
        loc=dma((2,)),
        tab_send=dma((owner_count,)),
        tab_recv=dma((owner_count,)),
        ring_send=dma((columns, halves)),
        ring_recv=dma((columns, halves)),
        **{name: dma((columns, plane)) for name in ("qs", "qr", "rs", "rr", "ls", "lr")},
        **{name: dma((columns, halves)) for name in ("ms", "mr", "mls", "mlr")},
        **{name: dma((parts,)) for name in ("ts", "tr", "xs", "xr")},
    )
    by_rows = pl.pallas_call(
        functools.partial(layer_kernel, (columns, plane, parts, local_heads, cap, pick_count, halves)),
        in_specs=[smem] + [vmem] * 6 + [hbm] * 8,
        out_specs=vmem,
        out_shape=jax.ShapeDtypeStruct((row_count // parts, parts * width), bf16),
        scratch_shapes=[scratch],
        compiler_params=pltpu.CompilerParams(
            collective_id=0, has_side_effects=True, vmem_limit_bytes=60 * 2**20
        ),
        name="layer",
    )(
        table,
        table.reshape(1, tab_size),
        token_gain.reshape(1, model),
        store_gain.reshape(1, model),
        spatial_gain.reshape(1, width),
        position_bias.T,
        position_mix,
        tokens,
        store,
        query_weight,
        spatial_weight,
        key_weight,
        read_weight,
        carry_weight,
        blend_weight,
    )
    return jnp.dot(by_rows, output_weight, preferred_element_type=f32).astype(bf16)


def solution(mesh):
    in_specs = (
        P("st", None),
        P("st", None),
        P("st", None, None),
        P(),
        P(),
        P(None, "tp"),
        P(None, "tp"),
        P("tp"),
        P("tp", None, None),
        P("tp", None),
        P(None, "tp"),
        P(None, "tp"),
        P(None, "tp"),
        P(None, "tp"),
        P(),
    )
    out_specs = P(("st", "tp"), None)
    return jax.shard_map(
        per_device, mesh=mesh, in_specs=in_specs, out_specs=out_specs, check_vma=False
    )
```

```python
import functools

import jax
import jax.numpy as jnp
from jax import lax
from jax.experimental import pallas as pl
from jax.experimental.pallas import tpu as pltpu
from jax.sharding import PartitionSpec as P

norm_eps = 1e-06
bf16 = jnp.bfloat16
f32 = jnp.float32


def normed_rows(matrix, gain):
    values = matrix.astype(f32)
    scaled = values * lax.rsqrt(jnp.mean(values * values, axis=-1, keepdims=True) + norm_eps)
    return (scaled * gain).astype(bf16)

far = -1e30
MESH = pl.DeviceIdType.MESH


def stacked_queries(q, heads):
    length, width = q.shape
    dim = width // heads
    row_head = lax.broadcasted_iota(jnp.int32, (heads * length, width), 0) // length
    lane_head = lax.broadcasted_iota(jnp.int32, (heads * length, width), 1) // dim
    return jnp.where(row_head == lane_head, jnp.concatenate([q] * heads, axis=0), jnp.zeros((), bf16))


def own_head(o, heads):
    width, columns = o.shape
    dim, length = width // heads, columns // heads
    col_head = lax.broadcasted_iota(jnp.int32, (dim, columns), 1) // length
    out = o[0:dim]
    for h in range(1, heads):
        out = jnp.where(col_head == h, o[h * dim : (h + 1) * dim], out)
    return out


def erf_gelu(x):
    return 0.5 * x * (1.0 + lax.erf(x * 0.5**0.5))


def fill_table(ids_ref, tab_ref, n, cap, count):
    picks, spans = ids_ref.shape
    requests = spans * picks
    i32 = jnp.int32
    wide = tab_ref.shape[1] - 2 * (-(-n * cap // 128) * 128)
    lane = lax.broadcasted_iota(i32, (picks, wide), 1)
    pick = lax.broadcasted_iota(i32, (picks, wide), 0)
    spread = jnp.zeros((picks, wide), i32)
    for s in range(spans):
        spread = spread + jnp.where(lane == s * picks + pick, ids_ref[:, s : s + 1], 0)
    ids = sum(spread[k : k + 1] for k in range(picks))
    lane = lane[0:1]
    owner = jnp.zeros((1, wide), i32)
    for o in range(1, n):
        owner = owner + jnp.where(ids >= o * count, 1, 0)
    inside = ids - owner * count
    span = jnp.zeros((1, wide), i32)
    for s in range(1, spans):
        span = span + jnp.where(lane >= s * picks, 1, 0)
    owner = jnp.where(lane < requests, owner, n)

    def down(row):
        return jnp.broadcast_to(row, (wide, wide)).T

    row_of = lax.broadcasted_iota(i32, (wide, wide), 0)
    lane_of = lax.broadcasted_iota(i32, (wide, wide), 1)
    earlier = (down(owner) == owner) & (row_of < lane_of)
    position = owner * cap + jnp.sum(jnp.where(earlier, 1, 0), axis=0, keepdims=True)
    place, inside, span = down(position), down(inside), down(span)
    section = (tab_ref.shape[1] - wide) // 2
    for b in range(0, section, wide):
        hit = (place == lane_of + b) & (row_of < requests)
        tab_ref[:, b : b + wide] = jnp.sum(jnp.where(hit, inside, 0), axis=0, keepdims=True)
        tab_ref[:, section + b : section + b + wide] = jnp.sum(jnp.where(hit, span, 0), axis=0, keepdims=True)
    tab_ref[:, 2 * section :] = position


def layer_kernel(
    sizes,
    ids_ref,
    token_gain,
    store_gain,
    spatial_gain,
    bias_ref,
    mix_ref,
    tokens,
    store,
    wq,
    ws,
    wk,
    wv,
    wc,
    wb,
    out_ref,
    v,
):
    columns, plane, parts, heads, cap, picks, halves = sizes
    q_own, qcol, qout, qin = v["q_own"], v["qcol"], v["qout"], v["qin"]
    rout, lout, rin, lin = v["rout"], v["lout"], v["rin"], v["lin"]
    mout, mlout, mid, mlin, half = v["mout"], v["mlout"], v["mid"], v["mlin"], v["half"]
    tab_ref, own_tab = v["tab"], v["own_tab"]
    tabs_v, tabs_s, normed = v["tabs_v"], v["tabs_s"], v["normed"]
    keys, values_t, w_ref = v["keys"], v["values_t"], v["w"]
    n = columns * plane
    spans, length, width = q_own.shape
    tiles, tile, model = normed.shape
    per = tile // length
    store_count = keys.shape[0]
    dim = width // heads
    scale = dim ** (-0.5)
    slots = n * cap
    section = -(-slots // 128) * 128
    local = plane * cap
    me = lax.axis_index("st")
    side = lax.axis_index("tp")
    z = me // plane
    p = me % plane
    base = z * local
    following = {"st": lax.rem(z + 1, columns) * plane + p}
    group = spans // halves

    def each(count, f, first=0):
        def body(i, carry):
            f(i)
            return carry

        lax.fori_loop(first, count, body, 0)

    def remote(src, dst, send, recv, where):
        return pltpu.make_async_remote_copy(
            src_ref=src, dst_ref=dst, send_sem=send, recv_sem=recv, device_id=where, device_id_type=MESH
        )

    def token_copy(i):
        rows = pl.ds(pl.multiple_of(i * tile, tile), tile)
        return pltpu.make_async_copy(tokens.at[rows], v["tok"].at[i], v["tok_sem"].at[i])

    def store_copy(i):
        return pltpu.make_async_copy(store.at[i], v["st"].at[i], v["st_sem"].at[i])

    def weight_copy(i):
        return pltpu.make_async_copy((wq, ws, wk, wv, wc, wb)[i], w_ref.at[i], v["w_sem"].at[i])

    def mate(j):
        return {"st": z * plane + lax.rem(p + j, plane)}

    def back_mate(j):
        return {"st": z * plane + lax.rem(p + plane - j, plane)}

    def other(d):
        return {"tp": lax.rem(side + d, parts)}

    def tab_copy(d):
        return remote(tab_ref, tabs_v.at[me], v["tab_send"].at[d], v["tab_recv"].at[d], {"st": lax.rem(me + d, n)})

    def block(s):
        return q_own if s == 0 else qcol[s - 1]

    def ring_copy(s, h):
        piece = pl.ds(h * (spans // halves), spans // halves)
        send, recv = v["ring_send"].at[s, h], v["ring_recv"].at[s, h]
        return remote(block(s).at[piece], qcol[s].at[piece], send, recv, following)

    def query_copy(s, j):
        return remote(qout.at[s, j], qin.at[s, j], v["qs"].at[s, j], v["qr"].at[s, j], mate(j))

    def result_copies(s, j):
        mine = pl.ds(p * cap, cap)
        return (
            remote(rout.at[s, j], rin[s].at[mine], v["rs"].at[s, j], v["rr"].at[s, j], back_mate(j)),
            remote(lout.at[s, j], lin[s].at[mine], v["ls"].at[s, j], v["lr"].at[s, j], back_mate(j)),
        )

    def merged_copies(s, h):
        i = s - 1
        return (
            remote(mout.at[i, h], mid.at[i, h], v["ms"].at[i, h], v["mr"].at[i, h], following),
            remote(mlout.at[i, h], mlin.at[i, h], v["mls"].at[i, h], v["mlr"].at[i, h], following),
        )

    def moment_copy(d):
        return remote(v["mom"], v["mom_in"].at[d - 1], v["xs"].at[d - 1], v["xr"].at[d - 1], other(d))

    def look(s, j, i):
        row = lax.rem(z + columns - s, columns) * plane + lax.rem(p + plane - j, plane)
        return tabs_s[row, 0, i]

    weight_copy(0).start()
    each(tiles, lambda i: token_copy(i).start())

    barrier = pltpu.get_barrier_semaphore()

    def greet(d):
        pl.semaphore_signal(barrier, inc=1, device_id={"st": lax.rem(me + d, n)}, device_id_type=MESH)

    each(n, greet, 1)
    for d in range(1, parts):
        pl.semaphore_signal(barrier, inc=1, device_id=other(d), device_id_type=MESH)

    fill_table(ids_ref, tab_ref, n, cap, store_count)
    weight_copy(0).wait()

    def query(i):
        token_copy(i).wait()
        rows = normed_rows(v["tok"][i], token_gain[...])
        normed[i] = rows
        q = jnp.dot(rows, w_ref[0], preferred_element_type=f32).astype(bf16)
        for s in range(per):
            q_own[i * per + s] = q[s * length : (s + 1) * length]

    for h in range(halves):
        each(tiles * (h + 1) // halves, query, tiles * h // halves)
        if h == 0:
            table_copy = pltpu.make_async_copy(tab_ref, own_tab, v["loc"].at[2])
            table_copy.start()
            pl.semaphore_wait(barrier, n - 1 + parts - 1)
        if columns > 1:
            ring_copy(0, h).start()
    each(n, lambda d: tab_copy(d).start(), 1)
    own_copy = pltpu.make_async_copy(tab_ref, tabs_v.at[me], v["loc"].at[0])
    own_copy.start()
    for i in range(1, 6):
        weight_copy(i).start()
    each(store_count, lambda i: store_copy(i).start())
    table_copy.wait()

    def select(s):
        def pick(j):
            o = z * plane + lax.rem(p + j, plane)
            for c in range(cap):
                i = section + o * cap + c
                span = own_tab[0, i] if s == 0 else look(s, 0, i)
                qout[s, j, c] = block(s)[span]

        each(plane, pick, 1)
        each(plane, lambda j: query_copy(s, j).start(), 1)

    select(0)

    def spatial_first(i):
        x = jnp.dot(normed[i], w_ref[1], preferred_element_type=f32)
        x = erf_gelu(x)
        v["spatial"][i] = x
        one = jnp.sum(x, axis=1, keepdims=True)
        two = jnp.sum(x * x, axis=1, keepdims=True)
        lane = lax.broadcasted_iota(jnp.int32, (tile, 128), 1)
        v["mom"][i] = jnp.where(lane < 64, one, two)

    weight_copy(1).wait()
    each(tiles, spatial_first)
    for d in range(1, parts):
        moment_copy(d).start()

    def project(i):
        store_copy(i).wait()
        rows = normed_rows(v["st"][i], store_gain[...])
        keys[i] = jnp.dot(rows, w_ref[2], preferred_element_type=f32).astype(bf16)
        values_t[i] = jnp.dot(rows, w_ref[3], preferred_element_type=f32).T.astype(bf16)

    def spatial_rest():
        for d in range(1, parts):
            moment_copy(d).wait_recv()
        weight_copy(4).wait()
        weight_copy(5).wait()

        def one(i):
            mom = v["mom"][i]
            for d in range(1, parts):
                mom = mom + v["mom_in"][d - 1, i]
            mom = mom / (width * parts)
            mean = mom[:, 0:1]
            spread = mom[:, 64:65] - mean * mean
            x = (v["spatial"][i] - mean) * lax.rsqrt(spread + norm_eps) * spatial_gain[...]
            x = x.astype(bf16)
            bias = jnp.concatenate([bias_ref[...]] * (-(-8 // heads)), axis=0).T
            mixed = [
                jnp.dot(mix_ref[h], x[:, h * dim : (h + 1) * dim], preferred_element_type=f32)
                + bias[:, h : h + 1]
                for h in range(heads)
            ]
            mixed = jnp.concatenate(mixed, axis=1)
            carry = jnp.dot(normed[i], w_ref[4], preferred_element_type=f32)
            v["gated"][i] = erf_gelu(carry) * mixed
            v["blend"][i] = jax.nn.sigmoid(jnp.dot(normed[i], w_ref[5], preferred_element_type=f32))

        each(tiles, one)

    def attend(queries, passages, put):
        for c in range(cap):
            v["s"][c] = (
                lax.dot_general(
                    keys[passages[c]],
                    stacked_queries(queries[c], heads),
                    (((1,), (1,)), ((), ())),
                    preferred_element_type=f32,
                )
                * scale
            )
        totals = []
        levels = []
        for c in range(cap):
            s = v["s"][c]
            peak = jnp.max(s, axis=0, keepdims=True)
            w = jnp.exp(s - peak)
            total = jnp.sum(w, axis=0, keepdims=True)
            v["p"][c] = w.astype(bf16)
            totals.append(total)
            levels.append(peak + jnp.log(total))
        for c in range(cap):
            o = jnp.dot(values_t[passages[c]], v["p"][c], preferred_element_type=f32)
            put(c, (own_head(o, heads) / totals[c]).astype(bf16), levels[c])

    def send_results(s, j):
        for copy in result_copies(s, j):
            copy.start()

    def attention(s, send=True):
        mine = me * cap

        def for_mate(j):
            query_copy(s, j).wait_recv()

            def put(c, value, level):
                rout[s, j, c] = value
                lout[s, j, c] = level

            attend([qin[s, j, c] for c in range(cap)], [look(s, j, mine + c) for c in range(cap)], put)
            if send:

                @pl.when(j > 1)
                def _():
                    send_results(s, j - 1)

        each(plane, for_mate, 1)

        def put_here(c, value, level):
            rin[s][p * cap + c] = value
            lin[s][p * cap + c] = level

        here = [block(s)[look(s, 0, section + mine + c)] for c in range(cap)]
        if send and plane > 1:
            send_results(s, plane - 1)
        attend(here, [look(s, 0, mine + c) for c in range(cap)], put_here)

    def source(s, span, k):
        i = look(s, 0, 2 * section + span * picks + k) - base
        return jnp.clip(i, 0, local - 1), (i >= 0) & (i < local)

    def weigh(s, h, more):
        def one(i):
            for k in range(picks):
                at, inside = source(s, h * group + i, k)
                v["lev"][k, pl.ds(i, 1)] = jnp.where(inside, lin[s][at], far)

        each(group, one)
        levels = [v["lev"][k] for k in range(picks)] + more
        top = functools.reduce(jnp.maximum, levels)
        ws = [jnp.exp(level - top) for level in levels]
        total = sum(ws)
        for k, w in enumerate(ws):
            v["wt"][k] = w / total
        return top + jnp.log(total)

    def summed(s, h, i, more):
        at = pl.ds(i, 1)
        terms = [v["wt"][k, at] * rin[s][source(s, h * group + i, k)[0]].astype(f32) for k in range(picks)]
        for k, ref in enumerate(more):
            terms.append(v["wt"][picks + k, at] * ref[i].astype(f32))
        return sum(terms)

    def wait_results(s):
        def one(j):
            for copy in result_copies(s, j):
                copy.wait_recv()

        each(plane, one, 1)

    def arrived(s, h):
        if (s if s else columns) < 2:
            return [], []
        i = (s if s else columns) - 2
        for copy in merged_copies(i + 1, h):
            copy.wait_recv()
        return [mlin[i, h]], [mid.at[i, h]]

    def merge(s):
        wait_results(s)
        for d in range(1, halves + 1):
            h = lax.rem(side + d, halves)
            levels, blocks = arrived(s, h)
            mlout[s - 1, h] = weigh(s, h, levels)

            def one(i):
                mout[s - 1, h, i] = summed(s, h, i, blocks).astype(bf16)

            each(group, one)
            for copy in merged_copies(s, h):
                copy.start()

    own_copy.wait()
    weight_copy(2).wait()
    weight_copy(3).wait()
    steps = max(columns - 1, 1)
    cut = [store_count * min(i, 2) // 2 for i in range(steps + 1)] if steps > 1 else [0, store_count]
    for s in range(1, columns):
        each(cut[s], project, cut[s - 1])
        if s == 1:
            each(n, lambda d: tab_copy(d).wait_recv(), 1)
            to_smem = pltpu.make_async_copy(tabs_v, tabs_s, v["loc"].at[1])
            to_smem.start()
            to_smem.wait()
        for h in range(halves):
            ring_copy(s - 1, h).wait_recv()
            if s < columns - 1:
                ring_copy(s, h).start()
        select(s)
        if s > 1:
            attention(s - 1)
        if s == 2:
            spatial_rest()
    for s in range(1, columns - 1):
        merge(s)
        if s == 1:
            attention(0, False)
            attention(columns - 1)
            each(plane, lambda j: send_results(0, j), 1)
    if columns > 1:
        merge(columns - 1)
    wait_results(0)

    lanes = pl.ds(pl.multiple_of(side * width, width), width)

    def final(h, to):
        levels, blocks = arrived(0, h)
        weigh(0, h, levels)

        def one(i):
            span = h * group + i
            memory = summed(0, h, i, blocks).T
            memory = jnp.concatenate([memory[c * length : (c + 1) * length] for c in range(heads)], axis=1)
            at = pl.ds(pl.multiple_of(lax.rem(span, per) * length, length), length)
            t = span // per
            to(i, (v["gated"][t, at] + v["blend"][t, at] * memory).astype(bf16))

        each(group, one)

    def half_copy(d):
        i = d - 1
        return remote(half.at[i], out_ref.at[:, lanes], v["ts"].at[i], v["tr"].at[i], other(d))

    def rows_of(i):
        return pl.ds(pl.multiple_of(i * length, length), length)

    for d in range(1, parts):

        def keep(i, value):
            half[d - 1, rows_of(i)] = value

        final(lax.rem(side + d, parts), keep)
        half_copy(d).start()

    def keep_own(i, value):
        out_ref[rows_of(i), lanes] = value

    final(side, keep_own)

    for d in range(1, parts):
        half_copy(d).wait()
        moment_copy(d).wait_send()
    each(n, lambda d: tab_copy(d).wait_send(), 1)
    for s in range(columns - 1):
        for h in range(halves):
            ring_copy(s, h).wait_send()
    for s in range(columns):

        def done(j):
            query_copy(s, j).wait_send()
            for copy in result_copies(s, j):
                copy.wait_send()

        each(plane, done, 1)
    for s in range(1, columns):
        for h in range(halves):
            for copy in merged_copies(s, h):
                copy.wait_send()


def per_device(
    tokens,
    route_ids,
    store,
    token_gain,
    store_gain,
    carry_weight,
    spatial_weight,
    spatial_gain,
    position_mix,
    position_bias,
    query_weight,
    key_weight,
    read_weight,
    blend_weight,
    output_weight,
):
    row_count, model = tokens.shape
    local_heads, block_length = position_mix.shape[:2]
    width = carry_weight.shape[1]
    head_dim = width // local_heads
    span_count, pick_count = route_ids.shape
    span_length = row_count // span_count
    store_count, passage_length = store.shape[:2]
    owner_count = lax.axis_size("st")
    requests = span_count * pick_count
    cap = max(1, 2 * requests // owner_count)
    slots = owner_count * cap

    parts = lax.axis_size("tp")
    columns = 4 if owner_count % 4 == 0 else 1
    plane = owner_count // columns
    local = plane * cap
    wide = local_heads * span_length
    tiles = row_count // block_length
    halves = parts
    group = span_count // halves
    tab_size = 2 * (-(-owner_count * cap // 128) * 128) + (-(-requests // 128) * 128)
    vmem = pl.BlockSpec(memory_space=pltpu.VMEM)
    hbm = pl.BlockSpec(memory_space=pltpu.HBM)
    dma = pltpu.SemaphoreType.DMA
    V = pltpu.VMEM
    scratch = dict(
        tok=V((tiles, block_length, model), bf16),
        normed=V((tiles, block_length, model), bf16),
        st=V((store_count, passage_length, model), bf16),
        w=V((6, model, width), bf16),
        keys=V((store_count, passage_length, width), bf16),
        values_t=V((store_count, width, passage_length), bf16),
        spatial=V((tiles, block_length, width), f32),
        gated=V((tiles, block_length, width), f32),
        blend=V((tiles, block_length, width), f32),
        mom=V((tiles, block_length, 128), f32),
        mom_in=V((parts, tiles, block_length, 128), f32),
        tab=V((1, tab_size), jnp.int32),
        own_tab=pltpu.SMEM((1, tab_size), jnp.int32),
        tabs_v=V((owner_count, 1, tab_size), jnp.int32),
        tabs_s=pltpu.SMEM((owner_count, 1, tab_size), jnp.int32),
        q_own=V((span_count, span_length, width), bf16),
        qcol=[V((span_count, span_length, width), bf16)] * (columns - 1),
        qout=V((columns, plane, cap, span_length, width), bf16),
        qin=V((columns, plane, cap, span_length, width), bf16),
        rout=V((columns, plane, cap, head_dim, wide), bf16),
        lout=V((columns, plane, cap, 1, wide), f32),
        rin=[V((local, head_dim, wide), bf16)] * columns,
        lin=[V((local, 1, wide), f32)] * columns,
        mout=V((columns, halves, group, head_dim, wide), bf16),
        mlout=V((columns, halves, group, wide), f32),
        mid=V((columns, halves, group, head_dim, wide), bf16),
        mlin=V((columns, halves, group, wide), f32),
        lev=V((pick_count, group, wide), f32),
        wt=V((pick_count + 1, group, wide), f32),
        half=V((parts, row_count // parts, width), bf16),
        s=V((cap, passage_length, wide), f32),
        p=V((cap, passage_length, wide), bf16),
        tok_sem=dma((tiles,)),
        st_sem=dma((store_count,)),
        w_sem=dma((6,)),
        loc=dma((3,)),
        tab_send=dma((owner_count,)),
        tab_recv=dma((owner_count,)),
        ring_send=dma((columns, halves)),
        ring_recv=dma((columns, halves)),
        **{name: dma((columns, plane)) for name in ("qs", "qr", "rs", "rr", "ls", "lr")},
        **{name: dma((columns, halves)) for name in ("ms", "mr", "mls", "mlr")},
        **{name: dma((parts,)) for name in ("ts", "tr", "xs", "xr")},
    )
    by_rows = pl.pallas_call(
        functools.partial(layer_kernel, (columns, plane, parts, local_heads, cap, pick_count, halves)),
        in_specs=[vmem] * 6 + [hbm] * 8,
        out_specs=vmem,
        out_shape=jax.ShapeDtypeStruct((row_count // parts, parts * width), bf16),
        scratch_shapes=[scratch],
        compiler_params=pltpu.CompilerParams(
            collective_id=0, has_side_effects=True, vmem_limit_bytes=53 * 2**20
        ),
        name="layer",
    )(
        route_ids.T,
        token_gain.reshape(1, model),
        store_gain.reshape(1, model),
        spatial_gain.reshape(1, width),
        position_bias,
        position_mix,
        tokens,
        store,
        query_weight,
        spatial_weight,
        key_weight,
        read_weight,
        carry_weight,
        blend_weight,
    )
    return jnp.dot(by_rows, output_weight, preferred_element_type=f32).astype(bf16)


def solution(mesh):
    in_specs = (
        P("st", None),
        P("st", None),
        P("st", None, None),
        P(),
        P(),
        P(None, "tp"),
        P(None, "tp"),
        P("tp"),
        P("tp", None, None),
        P("tp", None),
        P(None, "tp"),
        P(None, "tp"),
        P(None, "tp"),
        P(None, "tp"),
        P(),
    )
    out_specs = P(("st", "tp"), None)
    return jax.shard_map(
        per_device, mesh=mesh, in_specs=in_specs, out_specs=out_specs, check_vma=False
    )
```

```python
import functools

import jax
import jax.numpy as jnp
from jax import lax
from jax.experimental import pallas as pl
from jax.experimental.pallas import tpu as pltpu
from jax.sharding import PartitionSpec as P

norm_eps = 1e-06
bf16 = jnp.bfloat16
f32 = jnp.float32


def normed_rows(matrix, gain):
    values = matrix.astype(f32)
    scaled = values * lax.rsqrt(jnp.mean(values * values, axis=-1, keepdims=True) + norm_eps)
    return (scaled * gain).astype(bf16)

far = -1e30
MESH = pl.DeviceIdType.MESH


def stacked_queries(q, heads):
    length, width = q.shape
    dim = width // heads
    row_head = lax.broadcasted_iota(jnp.int32, (heads * length, width), 0) // length
    lane_head = lax.broadcasted_iota(jnp.int32, (heads * length, width), 1) // dim
    return jnp.where(row_head == lane_head, jnp.concatenate([q] * heads, axis=0), jnp.zeros((), bf16))


def own_head(o, heads):
    width, columns = o.shape
    dim, length = width // heads, columns // heads
    col_head = lax.broadcasted_iota(jnp.int32, (dim, columns), 1) // length
    out = o[0:dim]
    for h in range(1, heads):
        out = jnp.where(col_head == h, o[h * dim : (h + 1) * dim], out)
    return out


def erf_gelu(x):
    return 0.5 * x * (1.0 + lax.erf(x * 0.5**0.5))


def fill_table(ids_ref, tab_ref, n, cap, count):
    picks, spans = ids_ref.shape
    requests = spans * picks
    i32 = jnp.int32
    wide = tab_ref.shape[1] - 2 * (-(-n * cap // 128) * 128)
    lane = lax.broadcasted_iota(i32, (picks, wide), 1)
    pick = lax.broadcasted_iota(i32, (picks, wide), 0)
    spread = jnp.zeros((picks, wide), i32)
    for s in range(spans):
        spread = spread + jnp.where(lane == s * picks + pick, ids_ref[:, s : s + 1], 0)
    ids = sum(spread[k : k + 1] for k in range(picks))
    lane = lane[0:1]
    owner = jnp.zeros((1, wide), i32)
    for o in range(1, n):
        owner = owner + jnp.where(ids >= o * count, 1, 0)
    inside = ids - owner * count
    span = jnp.zeros((1, wide), i32)
    for s in range(1, spans):
        span = span + jnp.where(lane >= s * picks, 1, 0)
    owner = jnp.where(lane < requests, owner, n)

    def down(row):
        return jnp.broadcast_to(row, (wide, wide)).T

    row_of = lax.broadcasted_iota(i32, (wide, wide), 0)
    lane_of = lax.broadcasted_iota(i32, (wide, wide), 1)
    earlier = (down(owner) == owner) & (row_of < lane_of)
    position = owner * cap + jnp.sum(jnp.where(earlier, 1, 0), axis=0, keepdims=True)
    place, inside, span = down(position), down(inside), down(span)
    section = (tab_ref.shape[1] - wide) // 2
    for b in range(0, section, wide):
        hit = (place == lane_of + b) & (row_of < requests)
        tab_ref[:, b : b + wide] = jnp.sum(jnp.where(hit, inside, 0), axis=0, keepdims=True)
        tab_ref[:, section + b : section + b + wide] = jnp.sum(jnp.where(hit, span, 0), axis=0, keepdims=True)
    tab_ref[:, 2 * section :] = position


def layer_kernel(
    sizes,
    ids_in,
    token_gain_in,
    store_gain_in,
    spatial_gain_in,
    bias_in,
    mix_in,
    tokens,
    store,
    wq,
    ws,
    wk,
    wv,
    wc,
    wb,
    out_ref,
    v,
):
    columns, plane, parts, heads, cap, picks, halves = sizes
    q_own, qcol, qout, qin = v["q_own"], v["qcol"], v["qout"], v["qin"]
    rout, lout, rin, lin = v["rout"], v["lout"], v["rin"], v["lin"]
    mout, mlout, mid, mlin, half = v["mout"], v["mlout"], v["mid"], v["mlin"], v["half"]
    tab_ref, own_tab = v["tab"], v["own_tab"]
    small = (ids_in, token_gain_in, store_gain_in, spatial_gain_in, bias_in, mix_in)
    ids_ref, token_gain, store_gain, spatial_gain, bias_ref, mix_ref = v["small"]
    tabs_v, tabs_s, normed = v["tabs_v"], v["tabs_s"], v["normed"]
    keys, values_t, w_ref = v["keys"], v["values_t"], v["w"]
    n = columns * plane
    spans, length, width = q_own.shape
    tiles, tile, model = normed.shape
    per = tile // length
    store_count = keys.shape[0]
    dim = width // heads
    scale = dim ** (-0.5)
    slots = n * cap
    section = -(-slots // 128) * 128
    local = plane * cap
    me = lax.axis_index("st")
    side = lax.axis_index("tp")
    z = me // plane
    p = me % plane
    base = z * local
    following = {"st": lax.rem(z + 1, columns) * plane + p}
    group = spans // halves

    def each(count, f, first=0):
        def body(i, carry):
            f(i)
            return carry

        lax.fori_loop(first, count, body, 0)

    def remote(src, dst, send, recv, where):
        return pltpu.make_async_remote_copy(
            src_ref=src, dst_ref=dst, send_sem=send, recv_sem=recv, device_id=where, device_id_type=MESH
        )

    def token_copy(i):
        rows = pl.ds(pl.multiple_of(i * tile, tile), tile)
        return pltpu.make_async_copy(tokens.at[rows], v["tok"].at[i], v["tok_sem"].at[i])

    def store_copy(i):
        return pltpu.make_async_copy(store.at[i], v["st"].at[i], v["st_sem"].at[i])

    def weight_copy(i):
        return pltpu.make_async_copy((wq, ws, wk, wv, wc, wb)[i], w_ref.at[i], v["w_sem"].at[i])

    def mate(j):
        return {"st": z * plane + lax.rem(p + j, plane)}

    def back_mate(j):
        return {"st": z * plane + lax.rem(p + plane - j, plane)}

    def other(d):
        return {"tp": lax.rem(side + d, parts)}

    def tab_copy(d):
        return remote(tab_ref, tabs_v.at[me], v["tab_send"].at[d], v["tab_recv"].at[d], {"st": lax.rem(me + d, n)})

    def block(s):
        return q_own if s == 0 else qcol[s - 1]

    def ring_copy(s, h):
        piece = pl.ds(h * (spans // halves), spans // halves)
        send, recv = v["ring_send"].at[s, h], v["ring_recv"].at[s, h]
        return remote(block(s).at[piece], qcol[s].at[piece], send, recv, following)

    def query_copy(s, j):
        return remote(qout.at[s, j], qin.at[s, j], v["qs"].at[s, j], v["qr"].at[s, j], mate(j))

    def result_copies(s, j):
        mine = pl.ds(p * cap, cap)
        return (
            remote(rout.at[s, j], rin[s].at[mine], v["rs"].at[s, j], v["rr"].at[s, j], back_mate(j)),
            remote(lout.at[s, j], lin[s].at[mine], v["ls"].at[s, j], v["lr"].at[s, j], back_mate(j)),
        )

    def merged_copies(s, h):
        i = s - 1
        return (
            remote(mout.at[i, h], mid.at[i, h], v["ms"].at[i, h], v["mr"].at[i, h], following),
            remote(mlout.at[i, h], mlin.at[i, h], v["mls"].at[i, h], v["mlr"].at[i, h], following),
        )

    def moment_copy(d):
        return remote(v["mom"], v["mom_in"].at[d - 1], v["xs"].at[d - 1], v["xr"].at[d - 1], other(d))

    def look(s, j, i):
        row = lax.rem(z + columns - s, columns) * plane + lax.rem(p + plane - j, plane)
        return tabs_s[row, 0, i]

    def small_copy(i):
        return pltpu.make_async_copy(small[i], v["small"][i], v["small_sem"].at[i])

    small_copy(0).start()
    small_copy(1).start()
    weight_copy(0).start()
    each(tiles, lambda i: token_copy(i).start())
    for i in range(2, 6):
        small_copy(i).start()

    barrier = pltpu.get_barrier_semaphore()

    def greet(d):
        pl.semaphore_signal(barrier, inc=1, device_id={"st": lax.rem(me + d, n)}, device_id_type=MESH)

    each(n, greet, 1)
    for d in range(1, parts):
        pl.semaphore_signal(barrier, inc=1, device_id=other(d), device_id_type=MESH)

    small_copy(0).wait()
    fill_table(ids_ref, tab_ref, n, cap, store_count)
    small_copy(1).wait()
    weight_copy(0).wait()

    def query(i):
        token_copy(i).wait()
        rows = normed_rows(v["tok"][i], token_gain[...])
        normed[i] = rows
        q = jnp.dot(rows, w_ref[0], preferred_element_type=f32).astype(bf16)
        for s in range(per):
            q_own[i * per + s] = q[s * length : (s + 1) * length]

    for h in range(halves):
        each(tiles * (h + 1) // halves, query, tiles * h // halves)
        if h == 0:
            table_copy = pltpu.make_async_copy(tab_ref, own_tab, v["loc"].at[2])
            table_copy.start()
            pl.semaphore_wait(barrier, n - 1 + parts - 1)
        if columns > 1:
            ring_copy(0, h).start()
    each(n, lambda d: tab_copy(d).start(), 1)
    own_copy = pltpu.make_async_copy(tab_ref, tabs_v.at[me], v["loc"].at[0])
    own_copy.start()
    for i in range(1, 6):
        weight_copy(i).start()
    each(store_count, lambda i: store_copy(i).start())
    for i in range(2, 6):
        small_copy(i).wait()
    table_copy.wait()

    def select(s):
        def pick(j):
            o = z * plane + lax.rem(p + j, plane)
            for c in range(cap):
                i = section + o * cap + c
                span = own_tab[0, i] if s == 0 else look(s, 0, i)
                qout[s, j, c] = block(s)[span]

        each(plane, pick, 1)
        each(plane, lambda j: query_copy(s, j).start(), 1)

    select(0)

    def spatial_first(i):
        x = jnp.dot(normed[i], w_ref[1], preferred_element_type=f32)
        x = erf_gelu(x)
        v["spatial"][i] = x
        one = jnp.sum(x, axis=1, keepdims=True)
        two = jnp.sum(x * x, axis=1, keepdims=True)
        lane = lax.broadcasted_iota(jnp.int32, (tile, 128), 1)
        v["mom"][i] = jnp.where(lane < 64, one, two)

    weight_copy(1).wait()
    each(tiles, spatial_first)
    for d in range(1, parts):
        moment_copy(d).start()

    def project(i):
        store_copy(i).wait()
        rows = normed_rows(v["st"][i], store_gain[...])
        keys[i] = jnp.dot(rows, w_ref[2], preferred_element_type=f32).astype(bf16)
        values_t[i] = jnp.dot(rows, w_ref[3], preferred_element_type=f32).T.astype(bf16)

    def spatial_rest():
        for d in range(1, parts):
            moment_copy(d).wait_recv()
        weight_copy(4).wait()
        weight_copy(5).wait()

        def one(i):
            mom = v["mom"][i]
            for d in range(1, parts):
                mom = mom + v["mom_in"][d - 1, i]
            mom = mom / (width * parts)
            mean = mom[:, 0:1]
            spread = mom[:, 64:65] - mean * mean
            x = (v["spatial"][i] - mean) * lax.rsqrt(spread + norm_eps) * spatial_gain[...]
            x = x.astype(bf16)
            bias = jnp.concatenate([bias_ref[...]] * (-(-8 // heads)), axis=0).T
            mixed = [
                jnp.dot(mix_ref[h], x[:, h * dim : (h + 1) * dim], preferred_element_type=f32)
                + bias[:, h : h + 1]
                for h in range(heads)
            ]
            mixed = jnp.concatenate(mixed, axis=1)
            carry = jnp.dot(normed[i], w_ref[4], preferred_element_type=f32)
            v["gated"][i] = erf_gelu(carry) * mixed
            v["blend"][i] = jax.nn.sigmoid(jnp.dot(normed[i], w_ref[5], preferred_element_type=f32))

        each(tiles, one)

    def attend(queries, passages, put):
        for c in range(cap):
            v["s"][c] = (
                lax.dot_general(
                    keys[passages[c]],
                    stacked_queries(queries[c], heads),
                    (((1,), (1,)), ((), ())),
                    preferred_element_type=f32,
                )
                * scale
            )
        totals = []
        levels = []
        for c in range(cap):
            s = v["s"][c]
            peak = jnp.max(s, axis=0, keepdims=True)
            w = jnp.exp(s - peak)
            total = jnp.sum(w, axis=0, keepdims=True)
            v["p"][c] = w.astype(bf16)
            totals.append(total)
            levels.append(peak + jnp.log(total))
        for c in range(cap):
            o = jnp.dot(values_t[passages[c]], v["p"][c], preferred_element_type=f32)
            put(c, (own_head(o, heads) / totals[c]).astype(bf16), levels[c])

    def send_results(s, j):
        for copy in result_copies(s, j):
            copy.start()

    def attention(s, send=True):
        mine = me * cap

        def for_mate(j):
            query_copy(s, j).wait_recv()

            def put(c, value, level):
                rout[s, j, c] = value
                lout[s, j, c] = level

            attend([qin[s, j, c] for c in range(cap)], [look(s, j, mine + c) for c in range(cap)], put)
            if send:

                @pl.when(j > 1)
                def _():
                    send_results(s, j - 1)

        each(plane, for_mate, 1)

        def put_here(c, value, level):
            rin[s][p * cap + c] = value
            lin[s][p * cap + c] = level

        here = [block(s)[look(s, 0, section + mine + c)] for c in range(cap)]
        if send and plane > 1:
            send_results(s, plane - 1)
        attend(here, [look(s, 0, mine + c) for c in range(cap)], put_here)

    def source(s, span, k):
        i = look(s, 0, 2 * section + span * picks + k) - base
        return jnp.clip(i, 0, local - 1), (i >= 0) & (i < local)

    def weigh(s, h, more):
        def one(i):
            for k in range(picks):
                at, inside = source(s, h * group + i, k)
                v["lev"][k, pl.ds(i, 1)] = jnp.where(inside, lin[s][at], far)

        each(group, one)
        levels = [v["lev"][k] for k in range(picks)] + more
        top = functools.reduce(jnp.maximum, levels)
        ws = [jnp.exp(level - top) for level in levels]
        total = sum(ws)
        for k, w in enumerate(ws):
            v["wt"][k] = w / total
        return top + jnp.log(total)

    def summed(s, h, i, more):
        at = pl.ds(i, 1)
        terms = [v["wt"][k, at] * rin[s][source(s, h * group + i, k)[0]].astype(f32) for k in range(picks)]
        for k, ref in enumerate(more):
            terms.append(v["wt"][picks + k, at] * ref[i].astype(f32))
        return sum(terms)

    def wait_results(s):
        def one(j):
            for copy in result_copies(s, j):
                copy.wait_recv()

        each(plane, one, 1)

    def arrived(s, h):
        if (s if s else columns) < 2:
            return [], []
        i = (s if s else columns) - 2
        for copy in merged_copies(i + 1, h):
            copy.wait_recv()
        return [mlin[i, h]], [mid.at[i, h]]

    def merge(s):
        wait_results(s)
        for d in range(1, halves + 1):
            h = lax.rem(side + d, halves)
            levels, blocks = arrived(s, h)
            mlout[s - 1, h] = weigh(s, h, levels)

            def one(i):
                mout[s - 1, h, i] = summed(s, h, i, blocks).astype(bf16)

            each(group, one)
            for copy in merged_copies(s, h):
                copy.start()

    own_copy.wait()
    weight_copy(2).wait()
    weight_copy(3).wait()
    cuts = [store_count * part // 24 for part in (0, 3, 8, 14, 20, 24)]
    if columns == 1:
        each(store_count, project)
    for s in range(1, columns):
        for h in range(halves):
            k = (s - 1) * halves + h
            if k + 1 < len(cuts):
                each(cuts[k + 1], project, cuts[k])
            if k == 0:
                each(n, lambda d: tab_copy(d).wait_recv(), 1)
                to_smem = pltpu.make_async_copy(tabs_v, tabs_s, v["loc"].at[1])
                to_smem.start()
                to_smem.wait()
            if s == columns - 1 and h == 0:
                for done in range(1, s - 1):
                    attention(done)
            ring_copy(s - 1, h).wait_recv()
            if s < columns - 1:
                ring_copy(s, h).start()
        select(s)
    spatial_rest()
    if columns > 1:
        attention(columns - 2)
    for s in range(1, columns - 1):
        merge(s)
        if s == 1:
            attention(0, False)
            attention(columns - 1)
            each(plane, lambda j: send_results(0, j), 1)
    if columns > 1:
        merge(columns - 1)
    wait_results(0)

    lanes = pl.ds(pl.multiple_of(side * width, width), width)

    def final(h, to):
        levels, blocks = arrived(0, h)
        weigh(0, h, levels)

        def one(i):
            span = h * group + i
            memory = summed(0, h, i, blocks).T
            memory = jnp.concatenate([memory[c * length : (c + 1) * length] for c in range(heads)], axis=1)
            at = pl.ds(pl.multiple_of(lax.rem(span, per) * length, length), length)
            t = span // per
            to(i, (v["gated"][t, at] + v["blend"][t, at] * memory).astype(bf16))

        each(group, one)

    def half_copy(d):
        i = d - 1
        return remote(half.at[i], out_ref.at[:, lanes], v["ts"].at[i], v["tr"].at[i], other(d))

    def rows_of(i):
        return pl.ds(pl.multiple_of(i * length, length), length)

    for d in range(1, parts):

        def keep(i, value):
            half[d - 1, rows_of(i)] = value

        final(lax.rem(side + d, parts), keep)
        half_copy(d).start()

    def keep_own(i, value):
        out_ref[rows_of(i), lanes] = value

    final(side, keep_own)

    for d in range(1, parts):
        half_copy(d).wait()
        moment_copy(d).wait_send()
    each(n, lambda d: tab_copy(d).wait_send(), 1)
    for s in range(columns - 1):
        for h in range(halves):
            ring_copy(s, h).wait_send()
    for s in range(columns):

        def done(j):
            query_copy(s, j).wait_send()
            for copy in result_copies(s, j):
                copy.wait_send()

        each(plane, done, 1)
    for s in range(1, columns):
        for h in range(halves):
            for copy in merged_copies(s, h):
                copy.wait_send()


def per_device(
    tokens,
    route_ids,
    store,
    token_gain,
    store_gain,
    carry_weight,
    spatial_weight,
    spatial_gain,
    position_mix,
    position_bias,
    query_weight,
    key_weight,
    read_weight,
    blend_weight,
    output_weight,
):
    row_count, model = tokens.shape
    local_heads, block_length = position_mix.shape[:2]
    width = carry_weight.shape[1]
    head_dim = width // local_heads
    span_count, pick_count = route_ids.shape
    span_length = row_count // span_count
    store_count, passage_length = store.shape[:2]
    owner_count = lax.axis_size("st")
    requests = span_count * pick_count
    cap = max(1, 2 * requests // owner_count)
    slots = owner_count * cap

    parts = lax.axis_size("tp")
    columns = 4 if owner_count % 4 == 0 else 1
    plane = owner_count // columns
    local = plane * cap
    wide = local_heads * span_length
    tiles = row_count // block_length
    halves = parts
    group = span_count // halves
    tab_size = 2 * (-(-owner_count * cap // 128) * 128) + (-(-requests // 128) * 128)
    vmem = pl.BlockSpec(memory_space=pltpu.VMEM)
    hbm = pl.BlockSpec(memory_space=pltpu.HBM)
    dma = pltpu.SemaphoreType.DMA
    V = pltpu.VMEM
    scratch = dict(
        tok=V((tiles, block_length, model), bf16),
        normed=V((tiles, block_length, model), bf16),
        st=V((store_count, passage_length, model), bf16),
        w=V((6, model, width), bf16),
        keys=V((store_count, passage_length, width), bf16),
        values_t=V((store_count, width, passage_length), bf16),
        spatial=V((tiles, block_length, width), f32),
        gated=V((tiles, block_length, width), f32),
        blend=V((tiles, block_length, width), f32),
        mom=V((tiles, block_length, 128), f32),
        mom_in=V((parts, tiles, block_length, 128), f32),
        small=[
            V((pick_count, span_count), jnp.int32),
            V((1, model), f32),
            V((1, model), f32),
            V((1, width), f32),
            V((local_heads, block_length), f32),
            V((local_heads, block_length, block_length), bf16),
        ],
        small_sem=dma((6,)),
        tab=V((1, tab_size), jnp.int32),
        own_tab=pltpu.SMEM((1, tab_size), jnp.int32),
        tabs_v=V((owner_count, 1, tab_size), jnp.int32),
        tabs_s=pltpu.SMEM((owner_count, 1, tab_size), jnp.int32),
        q_own=V((span_count, span_length, width), bf16),
        qcol=[V((span_count, span_length, width), bf16)] * (columns - 1),
        qout=V((columns, plane, cap, span_length, width), bf16),
        qin=V((columns, plane, cap, span_length, width), bf16),
        rout=V((columns, plane, cap, head_dim, wide), bf16),
        lout=V((columns, plane, cap, 1, wide), f32),
        rin=[V((local, head_dim, wide), bf16)] * columns,
        lin=[V((local, 1, wide), f32)] * columns,
        mout=V((columns, halves, group, head_dim, wide), bf16),
        mlout=V((columns, halves, group, wide), f32),
        mid=V((columns, halves, group, head_dim, wide), bf16),
        mlin=V((columns, halves, group, wide), f32),
        lev=V((pick_count, group, wide), f32),
        wt=V((pick_count + 1, group, wide), f32),
        half=V((parts, row_count // parts, width), bf16),
        s=V((cap, passage_length, wide), f32),
        p=V((cap, passage_length, wide), bf16),
        tok_sem=dma((tiles,)),
        st_sem=dma((store_count,)),
        w_sem=dma((6,)),
        loc=dma((3,)),
        tab_send=dma((owner_count,)),
        tab_recv=dma((owner_count,)),
        ring_send=dma((columns, halves)),
        ring_recv=dma((columns, halves)),
        **{name: dma((columns, plane)) for name in ("qs", "qr", "rs", "rr", "ls", "lr")},
        **{name: dma((columns, halves)) for name in ("ms", "mr", "mls", "mlr")},
        **{name: dma((parts,)) for name in ("ts", "tr", "xs", "xr")},
    )
    by_rows = pl.pallas_call(
        functools.partial(layer_kernel, (columns, plane, parts, local_heads, cap, pick_count, halves)),
        in_specs=[hbm] * 14,
        out_specs=vmem,
        out_shape=jax.ShapeDtypeStruct((row_count // parts, parts * width), bf16),
        scratch_shapes=[scratch],
        compiler_params=pltpu.CompilerParams(
            collective_id=0, has_side_effects=True, vmem_limit_bytes=60 * 2**20
        ),
        name="layer",
    )(
        route_ids.T,
        token_gain.reshape(1, model),
        store_gain.reshape(1, model),
        spatial_gain.reshape(1, width),
        position_bias,
        position_mix,
        tokens,
        store,
        query_weight,
        spatial_weight,
        key_weight,
        read_weight,
        carry_weight,
        blend_weight,
    )
    return jnp.dot(by_rows, output_weight, preferred_element_type=f32).astype(bf16)


def solution(mesh):
    in_specs = (
        P("st", None),
        P("st", None),
        P("st", None, None),
        P(),
        P(),
        P(None, "tp"),
        P(None, "tp"),
        P("tp"),
        P("tp", None, None),
        P("tp", None),
        P(None, "tp"),
        P(None, "tp"),
        P(None, "tp"),
        P(None, "tp"),
        P(),
    )
    out_specs = P(("st", "tp"), None)
    return jax.shard_map(
        per_device, mesh=mesh, in_specs=in_specs, out_specs=out_specs, check_vma=False
    )
```

```python
import functools

import jax
import jax.numpy as jnp
from jax import lax
from jax.experimental import pallas as pl
from jax.experimental.pallas import tpu as pltpu
from jax.sharding import PartitionSpec as P

norm_eps = 1e-06
bf16 = jnp.bfloat16
f32 = jnp.float32


def normed_rows(matrix, gain):
    values = matrix.astype(f32)
    scaled = values * lax.rsqrt(jnp.mean(values * values, axis=-1, keepdims=True) + norm_eps)
    return (scaled * gain).astype(bf16)

far = -1e30
MESH = pl.DeviceIdType.MESH


def stacked_queries(q, heads):
    length, width = q.shape
    dim = width // heads
    row_head = lax.broadcasted_iota(jnp.int32, (heads * length, width), 0) // length
    lane_head = lax.broadcasted_iota(jnp.int32, (heads * length, width), 1) // dim
    return jnp.where(row_head == lane_head, jnp.concatenate([q] * heads, axis=0), jnp.zeros((), bf16))


def own_head(o, heads):
    width, columns = o.shape
    dim, length = width // heads, columns // heads
    col_head = lax.broadcasted_iota(jnp.int32, (dim, columns), 1) // length
    out = o[0:dim]
    for h in range(1, heads):
        out = jnp.where(col_head == h, o[h * dim : (h + 1) * dim], out)
    return out


def erf_gelu(x):
    return 0.5 * x * (1.0 + lax.erf(x * 0.5**0.5))


def fill_table(ids_ref, tab_ref, n, cap, count):
    picks, spans = ids_ref.shape
    requests = spans * picks
    i32 = jnp.int32
    wide = tab_ref.shape[1] - 2 * (-(-n * cap // 128) * 128)
    lane = lax.broadcasted_iota(i32, (picks, wide), 1)
    pick = lax.broadcasted_iota(i32, (picks, wide), 0)
    spread = jnp.zeros((picks, wide), i32)
    for s in range(spans):
        spread = spread + jnp.where(lane == s * picks + pick, ids_ref[:, s : s + 1], 0)
    ids = sum(spread[k : k + 1] for k in range(picks))
    lane = lane[0:1]
    owner = jnp.zeros((1, wide), i32)
    for o in range(1, n):
        owner = owner + jnp.where(ids >= o * count, 1, 0)
    inside = ids - owner * count
    span = jnp.zeros((1, wide), i32)
    for s in range(1, spans):
        span = span + jnp.where(lane >= s * picks, 1, 0)
    owner = jnp.where(lane < requests, owner, n)

    def down(row):
        return jnp.broadcast_to(row, (wide, wide)).T

    row_of = lax.broadcasted_iota(i32, (wide, wide), 0)
    lane_of = lax.broadcasted_iota(i32, (wide, wide), 1)
    earlier = (down(owner) == owner) & (row_of < lane_of)
    position = owner * cap + jnp.sum(jnp.where(earlier, 1, 0), axis=0, keepdims=True)
    place, inside, span = down(position), down(inside), down(span)
    section = (tab_ref.shape[1] - wide) // 2
    for b in range(0, section, wide):
        hit = (place == lane_of + b) & (row_of < requests)
        tab_ref[:, b : b + wide] = jnp.sum(jnp.where(hit, inside, 0), axis=0, keepdims=True)
        tab_ref[:, section + b : section + b + wide] = jnp.sum(jnp.where(hit, span, 0), axis=0, keepdims=True)
    tab_ref[:, 2 * section :] = position


def layer_kernel(
    sizes,
    ids_in,
    token_gain_in,
    store_gain_in,
    spatial_gain_in,
    bias_in,
    mix_in,
    tokens,
    store,
    wq,
    ws,
    wk,
    wv,
    wc,
    wb,
    out_ref,
    v,
):
    columns, plane, parts, heads, cap, picks, halves = sizes
    q_own, qcol, qout, qin = v["q_own"], v["qcol"], v["qout"], v["qin"]
    rout, lout, rin, lin = v["rout"], v["lout"], v["rin"], v["lin"]
    mout, mlout, mid, mlin, half = v["mout"], v["mlout"], v["mid"], v["mlin"], v["half"]
    tab_ref, own_tab = v["tab"], v["own_tab"]
    small = (ids_in, token_gain_in, store_gain_in, spatial_gain_in, bias_in, mix_in)
    ids_ref, token_gain, store_gain, spatial_gain, bias_ref, mix_ref = v["small"]
    tabs_v, tabs_s, normed = v["tabs_v"], v["tabs_s"], v["normed"]
    keys, values_t, w_ref = v["keys"], v["values_t"], v["w"]
    n = columns * plane
    spans, length, width = q_own.shape
    tiles, tile, model = normed.shape
    per = tile // length
    store_count = keys.shape[0]
    dim = width // heads
    scale = dim ** (-0.5)
    slots = n * cap
    section = -(-slots // 128) * 128
    local = plane * cap
    me = lax.axis_index("st")
    side = lax.axis_index("tp")
    z = me // plane
    p = me % plane
    base = z * local
    following = {"st": lax.rem(z + 1, columns) * plane + p}
    group = spans // halves

    def each(count, f, first=0):
        def body(i, carry):
            f(i)
            return carry

        lax.fori_loop(first, count, body, 0)

    def remote(src, dst, send, recv, where):
        return pltpu.make_async_remote_copy(
            src_ref=src, dst_ref=dst, send_sem=send, recv_sem=recv, device_id=where, device_id_type=MESH
        )

    def token_copy(i):
        rows = pl.ds(pl.multiple_of(i * tile, tile), tile)
        return pltpu.make_async_copy(tokens.at[rows], v["tok"].at[i], v["tok_sem"].at[i])

    def store_copy(i):
        return pltpu.make_async_copy(store.at[i], v["st"].at[i], v["st_sem"].at[i])

    def weight_copy(i):
        return pltpu.make_async_copy((wq, ws, wk, wv, wc, wb)[i], w_ref.at[i], v["w_sem"].at[i])

    def mate(j):
        return {"st": z * plane + lax.rem(p + j, plane)}

    def back_mate(j):
        return {"st": z * plane + lax.rem(p + plane - j, plane)}

    def other(d):
        return {"tp": lax.rem(side + d, parts)}

    def tab_copy(d):
        return remote(tab_ref, tabs_v.at[me], v["tab_send"].at[d], v["tab_recv"].at[d], {"st": lax.rem(me + d, n)})

    def block(s):
        return q_own if s == 0 else qcol[s - 1]

    def ring_copy(s, h):
        piece = pl.ds(h * (spans // halves), spans // halves)
        send, recv = v["ring_send"].at[s, h], v["ring_recv"].at[s, h]
        return remote(block(s).at[piece], qcol[s].at[piece], send, recv, following)

    def query_copy(s, j):
        return remote(qout.at[s, j], qin.at[s, j], v["qs"].at[s, j], v["qr"].at[s, j], mate(j))

    def result_copies(s, j):
        mine = pl.ds(p * cap, cap)
        return (
            remote(rout.at[s, j], rin[s].at[mine], v["rs"].at[s, j], v["rr"].at[s, j], back_mate(j)),
            remote(lout.at[s, j], lin[s].at[mine], v["ls"].at[s, j], v["lr"].at[s, j], back_mate(j)),
        )

    def merged_copies(s, h):
        i = s - 1
        return (
            remote(mout.at[i, h], mid.at[i, h], v["ms"].at[i, h], v["mr"].at[i, h], following),
            remote(mlout.at[i, h], mlin.at[i, h], v["mls"].at[i, h], v["mlr"].at[i, h], following),
        )

    def moment_copy(d):
        return remote(v["mom"], v["mom_in"].at[d - 1], v["xs"].at[d - 1], v["xr"].at[d - 1], other(d))

    def look(s, j, i):
        row = lax.rem(z + columns - s, columns) * plane + lax.rem(p + plane - j, plane)
        return tabs_s[row, 0, i]

    def small_copy(i):
        return pltpu.make_async_copy(small[i], v["small"][i], v["small_sem"].at[i])

    small_copy(0).start()
    small_copy(1).start()
    weight_copy(0).start()
    each(tiles, lambda i: token_copy(i).start())
    for i in range(2, 6):
        small_copy(i).start()

    barrier = pltpu.get_barrier_semaphore()

    def greet(d):
        pl.semaphore_signal(barrier, inc=1, device_id={"st": lax.rem(me + d, n)}, device_id_type=MESH)

    each(n, greet, 1)
    for d in range(1, parts):
        pl.semaphore_signal(barrier, inc=1, device_id=other(d), device_id_type=MESH)

    small_copy(0).wait()
    fill_table(ids_ref, tab_ref, n, cap, store_count)
    small_copy(1).wait()
    weight_copy(0).wait()

    def query(i):
        token_copy(i).wait()
        rows = normed_rows(v["tok"][i], token_gain[...])
        normed[i] = rows
        q = jnp.dot(rows, w_ref[0], preferred_element_type=f32).astype(bf16)
        for s in range(per):
            q_own[i * per + s] = q[s * length : (s + 1) * length]

    for h in range(halves):
        each(tiles * (h + 1) // halves, query, tiles * h // halves)
        if h == 0:
            table_copy = pltpu.make_async_copy(tab_ref, own_tab, v["loc"].at[2])
            table_copy.start()
            pl.semaphore_wait(barrier, n - 1 + parts - 1)
        if columns > 1:
            ring_copy(0, h).start()
    each(n, lambda d: tab_copy(d).start(), 1)
    own_copy = pltpu.make_async_copy(tab_ref, tabs_v.at[me], v["loc"].at[0])
    own_copy.start()
    for i in range(1, 6):
        weight_copy(i).start()
    each(store_count, lambda i: store_copy(i).start())
    for i in range(2, 6):
        small_copy(i).wait()
    table_copy.wait()

    def select(s):
        def pick(j):
            o = z * plane + lax.rem(p + j, plane)
            for c in range(cap):
                i = section + o * cap + c
                span = own_tab[0, i] if s == 0 else look(s, 0, i)
                qout[s, j, c] = block(s)[span]

        each(plane, pick, 1)
        each(plane, lambda j: query_copy(s, j).start(), 1)

    select(0)

    def spatial_first(i):
        x = jnp.dot(normed[i], w_ref[1], preferred_element_type=f32)
        x = erf_gelu(x)
        v["spatial"][i] = x
        one = jnp.sum(x, axis=1, keepdims=True)
        two = jnp.sum(x * x, axis=1, keepdims=True)
        lane = lax.broadcasted_iota(jnp.int32, (tile, 128), 1)
        v["mom"][i] = jnp.where(lane < 64, one, two)

    weight_copy(1).wait()
    each(tiles, spatial_first)
    for d in range(1, parts):
        moment_copy(d).start()

    batch = 2 if store_count % 2 == 0 else 1
    passage = keys.shape[1]

    def project(i):
        for c in range(batch):
            store_copy(i * batch + c).wait()
        rows = [normed_rows(v["st"][i * batch + c], store_gain[...]) for c in range(batch)]
        rows = jnp.concatenate(rows, axis=0)
        k = jnp.dot(rows, w_ref[2], preferred_element_type=f32).astype(bf16)
        x = jnp.dot(rows, w_ref[3], preferred_element_type=f32)
        for c in range(batch):
            at = slice(c * passage, (c + 1) * passage)
            keys[i * batch + c] = k[at]
            values_t[i * batch + c] = x[at].T.astype(bf16)

    def spatial_rest():
        for d in range(1, parts):
            moment_copy(d).wait_recv()
        weight_copy(4).wait()
        weight_copy(5).wait()

        def one(i):
            mom = v["mom"][i]
            for d in range(1, parts):
                mom = mom + v["mom_in"][d - 1, i]
            mom = mom / (width * parts)
            mean = mom[:, 0:1]
            spread = mom[:, 64:65] - mean * mean
            x = (v["spatial"][i] - mean) * lax.rsqrt(spread + norm_eps) * spatial_gain[...]
            x = x.astype(bf16)
            bias = jnp.concatenate([bias_ref[...]] * (-(-8 // heads)), axis=0).T
            mixed = [
                jnp.dot(mix_ref[h], x[:, h * dim : (h + 1) * dim], preferred_element_type=f32)
                + bias[:, h : h + 1]
                for h in range(heads)
            ]
            mixed = jnp.concatenate(mixed, axis=1)
            carry = jnp.dot(normed[i], w_ref[4], preferred_element_type=f32)
            v["gated"][i] = erf_gelu(carry) * mixed
            v["blend"][i] = jax.nn.sigmoid(jnp.dot(normed[i], w_ref[5], preferred_element_type=f32))

        each(tiles, one)

    def attend(queries, passages, put):
        for c in range(cap):
            v["s"][c] = (
                lax.dot_general(
                    keys[passages[c]],
                    stacked_queries(queries[c], heads),
                    (((1,), (1,)), ((), ())),
                    preferred_element_type=f32,
                )
                * scale
            )
        totals = []
        levels = []
        for c in range(cap):
            s = v["s"][c]
            peak = jnp.max(s, axis=0, keepdims=True)
            w = jnp.exp(s - peak)
            total = jnp.sum(w, axis=0, keepdims=True)
            v["p"][c] = w.astype(bf16)
            totals.append(total)
            levels.append(peak + jnp.log(total))
        for c in range(cap):
            o = jnp.dot(values_t[passages[c]], v["p"][c], preferred_element_type=f32)
            put(c, (own_head(o, heads) / totals[c]).astype(bf16), levels[c])

    def send_results(s, j):
        for copy in result_copies(s, j):
            copy.start()

    def attention(s, send=True):
        mine = me * cap

        def for_mate(j):
            query_copy(s, j).wait_recv()

            def put(c, value, level):
                rout[s, j, c] = value
                lout[s, j, c] = level

            attend([qin[s, j, c] for c in range(cap)], [look(s, j, mine + c) for c in range(cap)], put)
            if send:

                @pl.when(j > 1)
                def _():
                    send_results(s, j - 1)

        each(plane, for_mate, 1)

        def put_here(c, value, level):
            rin[s][p * cap + c] = value
            lin[s][p * cap + c] = level

        here = [block(s)[look(s, 0, section + mine + c)] for c in range(cap)]
        if send and plane > 1:
            send_results(s, plane - 1)
        attend(here, [look(s, 0, mine + c) for c in range(cap)], put_here)

    def source(s, span, k):
        i = look(s, 0, 2 * section + span * picks + k) - base
        return jnp.clip(i, 0, local - 1), (i >= 0) & (i < local)

    def weigh(s, h, more):
        def one(i):
            for k in range(picks):
                at, inside = source(s, h * group + i, k)
                v["lev"][k, pl.ds(i, 1)] = jnp.where(inside, lin[s][at], far)

        each(group, one)
        levels = [v["lev"][k] for k in range(picks)] + more
        top = functools.reduce(jnp.maximum, levels)
        ws = [jnp.exp(level - top) for level in levels]
        total = sum(ws)
        for k, w in enumerate(ws):
            v["wt"][k] = w / total
        return top + jnp.log(total)

    def summed(s, h, i, more):
        at = pl.ds(i, 1)
        terms = [v["wt"][k, at] * rin[s][source(s, h * group + i, k)[0]].astype(f32) for k in range(picks)]
        for k, ref in enumerate(more):
            terms.append(v["wt"][picks + k, at] * ref[i].astype(f32))
        return sum(terms)

    def wait_results(s):
        def one(j):
            for copy in result_copies(s, j):
                copy.wait_recv()

        each(plane, one, 1)

    def arrived(s, h):
        if (s if s else columns) < 2:
            return [], []
        i = (s if s else columns) - 2
        for copy in merged_copies(i + 1, h):
            copy.wait_recv()
        return [mlin[i, h]], [mid.at[i, h]]

    def merge(s):
        wait_results(s)
        for d in range(1, halves + 1):
            h = lax.rem(side + d, halves)
            levels, blocks = arrived(s, h)
            mlout[s - 1, h] = weigh(s, h, levels)

            def one(i):
                mout[s - 1, h, i] = summed(s, h, i, blocks).astype(bf16)

            each(group, one)
            for copy in merged_copies(s, h):
                copy.start()

    own_copy.wait()
    weight_copy(2).wait()
    weight_copy(3).wait()
    cuts = [store_count // batch * part // 12 for part in (0, 1, 4, 7, 10, 12)]
    if columns == 1:
        each(store_count // batch, project)
    for s in range(1, columns):
        for h in range(halves):
            k = (s - 1) * halves + h
            if k + 1 < len(cuts):
                each(cuts[k + 1], project, cuts[k])
            if k == 0:
                each(n, lambda d: tab_copy(d).wait_recv(), 1)
                to_smem = pltpu.make_async_copy(tabs_v, tabs_s, v["loc"].at[1])
                to_smem.start()
                to_smem.wait()
            if s == columns - 1 and h == 0:
                for done in range(1, s - 1):
                    attention(done)
            ring_copy(s - 1, h).wait_recv()
            if s < columns - 1:
                ring_copy(s, h).start()
        select(s)
    spatial_rest()
    if columns > 1:
        attention(columns - 2)
    for s in range(1, columns - 1):
        merge(s)
        if s == 1:
            attention(0, False)
            attention(columns - 1)
            each(plane, lambda j: send_results(0, j), 1)
    if columns > 1:
        merge(columns - 1)
    wait_results(0)

    lanes = pl.ds(pl.multiple_of(side * width, width), width)

    def final(h, to):
        levels, blocks = arrived(0, h)
        weigh(0, h, levels)

        def one(i):
            span = h * group + i
            memory = summed(0, h, i, blocks).T
            memory = jnp.concatenate([memory[c * length : (c + 1) * length] for c in range(heads)], axis=1)
            at = pl.ds(pl.multiple_of(lax.rem(span, per) * length, length), length)
            t = span // per
            to(i, (v["gated"][t, at] + v["blend"][t, at] * memory).astype(bf16))

        each(group, one)

    def half_copy(d):
        i = d - 1
        return remote(half.at[i], out_ref.at[:, lanes], v["ts"].at[i], v["tr"].at[i], other(d))

    def rows_of(i):
        return pl.ds(pl.multiple_of(i * length, length), length)

    for d in range(1, parts):

        def keep(i, value):
            half[d - 1, rows_of(i)] = value

        final(lax.rem(side + d, parts), keep)
        half_copy(d).start()

    def keep_own(i, value):
        out_ref[rows_of(i), lanes] = value

    final(side, keep_own)

    for d in range(1, parts):
        half_copy(d).wait()
        moment_copy(d).wait_send()
    each(n, lambda d: tab_copy(d).wait_send(), 1)
    for s in range(columns - 1):
        for h in range(halves):
            ring_copy(s, h).wait_send()
    for s in range(columns):

        def done(j):
            query_copy(s, j).wait_send()
            for copy in result_copies(s, j):
                copy.wait_send()

        each(plane, done, 1)
    for s in range(1, columns):
        for h in range(halves):
            for copy in merged_copies(s, h):
                copy.wait_send()


def per_device(
    tokens,
    route_ids,
    store,
    token_gain,
    store_gain,
    carry_weight,
    spatial_weight,
    spatial_gain,
    position_mix,
    position_bias,
    query_weight,
    key_weight,
    read_weight,
    blend_weight,
    output_weight,
):
    row_count, model = tokens.shape
    local_heads, block_length = position_mix.shape[:2]
    width = carry_weight.shape[1]
    head_dim = width // local_heads
    span_count, pick_count = route_ids.shape
    span_length = row_count // span_count
    store_count, passage_length = store.shape[:2]
    owner_count = lax.axis_size("st")
    requests = span_count * pick_count
    cap = max(1, 2 * requests // owner_count)
    slots = owner_count * cap

    parts = lax.axis_size("tp")
    columns = 4 if owner_count % 4 == 0 else 1
    plane = owner_count // columns
    local = plane * cap
    wide = local_heads * span_length
    tiles = row_count // block_length
    halves = parts
    group = span_count // halves
    tab_size = 2 * (-(-owner_count * cap // 128) * 128) + (-(-requests // 128) * 128)
    vmem = pl.BlockSpec(memory_space=pltpu.VMEM)
    hbm = pl.BlockSpec(memory_space=pltpu.HBM)
    dma = pltpu.SemaphoreType.DMA
    V = pltpu.VMEM
    in_hbm = lambda x: pltpu.with_memory_space_constraint(x, pltpu.HBM)
    scratch = dict(
        tok=V((tiles, block_length, model), bf16),
        normed=V((tiles, block_length, model), bf16),
        st=V((store_count, passage_length, model), bf16),
        w=V((6, model, width), bf16),
        keys=V((store_count, passage_length, width), bf16),
        values_t=V((store_count, width, passage_length), bf16),
        spatial=V((tiles, block_length, width), f32),
        gated=V((tiles, block_length, width), f32),
        blend=V((tiles, block_length, width), f32),
        mom=V((tiles, block_length, 128), f32),
        mom_in=V((parts, tiles, block_length, 128), f32),
        small=[
            V((pick_count, span_count), jnp.int32),
            V((1, model), f32),
            V((1, model), f32),
            V((1, width), f32),
            V((local_heads, block_length), f32),
            V((local_heads, block_length, block_length), bf16),
        ],
        small_sem=dma((6,)),
        tab=V((1, tab_size), jnp.int32),
        own_tab=pltpu.SMEM((1, tab_size), jnp.int32),
        tabs_v=V((owner_count, 1, tab_size), jnp.int32),
        tabs_s=pltpu.SMEM((owner_count, 1, tab_size), jnp.int32),
        q_own=V((span_count, span_length, width), bf16),
        qcol=[V((span_count, span_length, width), bf16)] * (columns - 1),
        qout=V((columns, plane, cap, span_length, width), bf16),
        qin=V((columns, plane, cap, span_length, width), bf16),
        rout=V((columns, plane, cap, head_dim, wide), bf16),
        lout=V((columns, plane, cap, 1, wide), f32),
        rin=[V((local, head_dim, wide), bf16)] * columns,
        lin=[V((local, 1, wide), f32)] * columns,
        mout=V((columns, halves, group, head_dim, wide), bf16),
        mlout=V((columns, halves, group, wide), f32),
        mid=V((columns, halves, group, head_dim, wide), bf16),
        mlin=V((columns, halves, group, wide), f32),
        lev=V((pick_count, group, wide), f32),
        wt=V((pick_count + 1, group, wide), f32),
        half=V((parts, row_count // parts, width), bf16),
        s=V((cap, passage_length, wide), f32),
        p=V((cap, passage_length, wide), bf16),
        tok_sem=dma((tiles,)),
        st_sem=dma((store_count,)),
        w_sem=dma((6,)),
        loc=dma((3,)),
        tab_send=dma((owner_count,)),
        tab_recv=dma((owner_count,)),
        ring_send=dma((columns, halves)),
        ring_recv=dma((columns, halves)),
        **{name: dma((columns, plane)) for name in ("qs", "qr", "rs", "rr", "ls", "lr")},
        **{name: dma((columns, halves)) for name in ("ms", "mr", "mls", "mlr")},
        **{name: dma((parts,)) for name in ("ts", "tr", "xs", "xr")},
    )
    by_rows = pl.pallas_call(
        functools.partial(layer_kernel, (columns, plane, parts, local_heads, cap, pick_count, halves)),
        in_specs=[hbm] * 14,
        out_specs=vmem,
        out_shape=jax.ShapeDtypeStruct((row_count // parts, parts * width), bf16),
        scratch_shapes=[scratch],
        compiler_params=pltpu.CompilerParams(
            collective_id=0, has_side_effects=True, vmem_limit_bytes=53 * 2**20
        ),
        name="layer",
    )(
        in_hbm(route_ids.T),
        in_hbm(token_gain.reshape(1, model)),
        in_hbm(store_gain.reshape(1, model)),
        in_hbm(spatial_gain.reshape(1, width)),
        in_hbm(position_bias),
        in_hbm(position_mix),
        tokens,
        store,
        query_weight,
        spatial_weight,
        key_weight,
        read_weight,
        carry_weight,
        blend_weight,
    )
    return jnp.dot(by_rows, output_weight, preferred_element_type=f32).astype(bf16)


def solution(mesh):
    in_specs = (
        P("st", None),
        P("st", None),
        P("st", None, None),
        P(),
        P(),
        P(None, "tp"),
        P(None, "tp"),
        P("tp"),
        P("tp", None, None),
        P("tp", None),
        P(None, "tp"),
        P(None, "tp"),
        P(None, "tp"),
        P(None, "tp"),
        P(),
    )
    out_specs = P(("st", "tp"), None)
    return jax.shard_map(
        per_device, mesh=mesh, in_specs=in_specs, out_specs=out_specs, check_vma=False
    )
```

```python
import functools

import jax
import jax.numpy as jnp
from jax import lax
from jax.experimental import pallas as pl
from jax.experimental.pallas import tpu as pltpu
from jax.sharding import PartitionSpec as P

norm_eps = 1e-06
bf16 = jnp.bfloat16
f32 = jnp.float32


def normed_rows(matrix, gain):
    values = matrix.astype(f32)
    scaled = values * lax.rsqrt(jnp.mean(values * values, axis=-1, keepdims=True) + norm_eps)
    return (scaled * gain).astype(bf16)

far = -1e30
MESH = pl.DeviceIdType.MESH


def stacked_queries(q, heads):
    length, width = q.shape
    dim = width // heads
    row_head = lax.broadcasted_iota(jnp.int32, (heads * length, width), 0) // length
    lane_head = lax.broadcasted_iota(jnp.int32, (heads * length, width), 1) // dim
    return jnp.where(row_head == lane_head, jnp.concatenate([q] * heads, axis=0), jnp.zeros((), bf16))


def own_head(o, heads):
    width, columns = o.shape
    dim, length = width // heads, columns // heads
    col_head = lax.broadcasted_iota(jnp.int32, (dim, columns), 1) // length
    out = o[0:dim]
    for h in range(1, heads):
        out = jnp.where(col_head == h, o[h * dim : (h + 1) * dim], out)
    return out


def erf_gelu(x):
    return 0.5 * x * (1.0 + lax.erf(x * 0.5**0.5))


def fill_table(ids_ref, tab_ref, n, cap, count):
    picks, spans = ids_ref.shape
    requests = spans * picks
    i32 = jnp.int32
    wide = tab_ref.shape[1] - 2 * (-(-n * cap // 128) * 128)
    lane = lax.broadcasted_iota(i32, (picks, wide), 1)
    pick = lax.broadcasted_iota(i32, (picks, wide), 0)
    spread = jnp.zeros((picks, wide), i32)
    for s in range(spans):
        spread = spread + jnp.where(lane == s * picks + pick, ids_ref[:, s : s + 1], 0)
    ids = sum(spread[k : k + 1] for k in range(picks))
    lane = lane[0:1]
    owner = jnp.zeros((1, wide), i32)
    for o in range(1, n):
        owner = owner + jnp.where(ids >= o * count, 1, 0)
    inside = ids - owner * count
    span = jnp.zeros((1, wide), i32)
    for s in range(1, spans):
        span = span + jnp.where(lane >= s * picks, 1, 0)
    owner = jnp.where(lane < requests, owner, n)

    def down(row):
        return jnp.broadcast_to(row, (wide, wide)).T

    row_of = lax.broadcasted_iota(i32, (wide, wide), 0)
    lane_of = lax.broadcasted_iota(i32, (wide, wide), 1)
    earlier = (down(owner) == owner) & (row_of < lane_of)
    position = owner * cap + jnp.sum(jnp.where(earlier, 1, 0), axis=0, keepdims=True)
    place, inside, span = down(position), down(inside), down(span)
    section = (tab_ref.shape[1] - wide) // 2
    for b in range(0, section, wide):
        hit = (place == lane_of + b) & (row_of < requests)
        tab_ref[:, b : b + wide] = jnp.sum(jnp.where(hit, inside, 0), axis=0, keepdims=True)
        tab_ref[:, section + b : section + b + wide] = jnp.sum(jnp.where(hit, span, 0), axis=0, keepdims=True)
    tab_ref[:, 2 * section :] = position


def layer_kernel(
    sizes,
    ids_in,
    token_gain_in,
    store_gain_in,
    spatial_gain_in,
    bias_in,
    mix_in,
    tokens,
    store,
    wq,
    ws,
    wk,
    wv,
    wc,
    wb,
    out_ref,
    v,
):
    columns, plane, parts, heads, cap, picks, halves = sizes
    q_own, qcol, qout, qin = v["q_own"], v["qcol"], v["qout"], v["qin"]
    rout, lout, rin, lin = v["rout"], v["lout"], v["rin"], v["lin"]
    mout, mlout, mid, mlin, half = v["mout"], v["mlout"], v["mid"], v["mlin"], v["half"]
    tab_ref, own_tab = v["tab"], v["own_tab"]
    small = (ids_in, token_gain_in, store_gain_in, spatial_gain_in, bias_in, mix_in)
    ids_ref, token_gain, store_gain, spatial_gain, bias_ref, mix_ref = v["small"]
    tabs_v, tabs_s, normed = v["tabs_v"], v["tabs_s"], v["normed"]
    keys, values_t, w_ref = v["keys"], v["values_t"], v["w"]
    n = columns * plane
    spans, length, width = q_own.shape
    tiles, tile, model = normed.shape
    per = tile // length
    store_count = keys.shape[0]
    dim = width // heads
    scale = dim ** (-0.5)
    slots = n * cap
    section = -(-slots // 128) * 128
    local = plane * cap
    me = lax.axis_index("st")
    side = lax.axis_index("tp")
    z = me // plane
    p = me % plane
    base = z * local
    following = {"st": lax.rem(z + 1, columns) * plane + p}
    group = spans // halves

    def each(count, f, first=0):
        def body(i, carry):
            f(i)
            return carry

        lax.fori_loop(first, count, body, 0)

    def unrolled(count, f, step=3):
        def some(i):
            for k in range(step):
                f(i * step + k)

        each(count // step, some)
        for k in range(count - count % step, count):
            f(k)

    def remote(src, dst, send, recv, where):
        return pltpu.make_async_remote_copy(
            src_ref=src, dst_ref=dst, send_sem=send, recv_sem=recv, device_id=where, device_id_type=MESH
        )

    def token_copy(i):
        rows = pl.ds(pl.multiple_of(i * tile, tile), tile)
        return pltpu.make_async_copy(tokens.at[rows], v["tok"].at[i], v["tok_sem"].at[i])

    def store_copy(i):
        return pltpu.make_async_copy(store.at[i], v["st"].at[i], v["st_sem"].at[i])

    def weight_copy(i):
        return pltpu.make_async_copy((wq, ws, wk, wv, wc, wb)[i], w_ref.at[i], v["w_sem"].at[i])

    def mate(j):
        return {"st": z * plane + lax.rem(p + j, plane)}

    def back_mate(j):
        return {"st": z * plane + lax.rem(p + plane - j, plane)}

    def other(d):
        return {"tp": lax.rem(side + d, parts)}

    def tab_copy(d):
        return remote(tab_ref, tabs_v.at[me], v["tab_send"].at[d], v["tab_recv"].at[d], {"st": lax.rem(me + d, n)})

    def block(s):
        return q_own if s == 0 else qcol[s - 1]

    def ring_copy(s, h):
        piece = pl.ds(h * (spans // halves), spans // halves)
        send, recv = v["ring_send"].at[s, h], v["ring_recv"].at[s, h]
        return remote(block(s).at[piece], qcol[s].at[piece], send, recv, following)

    def query_copy(s, j):
        return remote(qout.at[s, j], qin.at[s, j], v["qs"].at[s, j], v["qr"].at[s, j], mate(j))

    def result_copies(s, j):
        mine = pl.ds(p * cap, cap)
        return (
            remote(rout.at[s, j], rin[s].at[mine], v["rs"].at[s, j], v["rr"].at[s, j], back_mate(j)),
            remote(lout.at[s, j], lin[s].at[mine], v["ls"].at[s, j], v["lr"].at[s, j], back_mate(j)),
        )

    def merged_copies(s, h):
        i = s - 1
        return (
            remote(mout.at[i, h], mid.at[i, h], v["ms"].at[i, h], v["mr"].at[i, h], following),
            remote(mlout.at[i, h], mlin.at[i, h], v["mls"].at[i, h], v["mlr"].at[i, h], following),
        )

    def moment_copy(d):
        return remote(v["mom"], v["mom_in"].at[d - 1], v["xs"].at[d - 1], v["xr"].at[d - 1], other(d))

    def look(s, j, i):
        row = lax.rem(z + columns - s, columns) * plane + lax.rem(p + plane - j, plane)
        return tabs_s[row, 0, i]

    def small_copy(i):
        return pltpu.make_async_copy(small[i], v["small"][i], v["small_sem"].at[i])

    small_copy(0).start()
    small_copy(1).start()
    weight_copy(0).start()
    each(tiles, lambda i: token_copy(i).start())
    for i in range(2, 6):
        small_copy(i).start()

    barrier = pltpu.get_barrier_semaphore()

    def greet(d):
        pl.semaphore_signal(barrier, inc=1, device_id={"st": lax.rem(me + d, n)}, device_id_type=MESH)

    each(n, greet, 1)
    for d in range(1, parts):
        pl.semaphore_signal(barrier, inc=1, device_id=other(d), device_id_type=MESH)

    small_copy(0).wait()
    fill_table(ids_ref, tab_ref, n, cap, store_count)
    small_copy(1).wait()
    weight_copy(0).wait()

    def query(i):
        token_copy(i).wait()
        rows = normed_rows(v["tok"][i], token_gain[...])
        normed[i] = rows
        q = jnp.dot(rows, w_ref[0], preferred_element_type=f32).astype(bf16)
        for s in range(per):
            q_own[i * per + s] = q[s * length : (s + 1) * length]

    for h in range(halves):
        each(tiles * (h + 1) // halves, query, tiles * h // halves)
        if h == 0:
            table_copy = pltpu.make_async_copy(tab_ref, own_tab, v["loc"].at[2])
            table_copy.start()
            pl.semaphore_wait(barrier, n - 1 + parts - 1)
        if columns > 1:
            ring_copy(0, h).start()
    each(n, lambda d: tab_copy(d).start(), 1)
    own_copy = pltpu.make_async_copy(tab_ref, tabs_v.at[me], v["loc"].at[0])
    own_copy.start()
    for i in range(1, 6):
        weight_copy(i).start()
    each(store_count, lambda i: store_copy(i).start())
    for i in range(2, 6):
        small_copy(i).wait()
    table_copy.wait()

    def select(s):
        def pick(j):
            o = z * plane + lax.rem(p + j, plane)
            for c in range(cap):
                i = section + o * cap + c
                span = own_tab[0, i] if s == 0 else look(s, 0, i)
                qout[s, j, c] = block(s)[span]

        each(plane, pick, 1)
        each(plane, lambda j: query_copy(s, j).start(), 1)

    select(0)

    def spatial_first(i):
        x = jnp.dot(normed[i], w_ref[1], preferred_element_type=f32)
        x = erf_gelu(x)
        v["spatial"][i] = x
        one = jnp.sum(x, axis=1, keepdims=True)
        two = jnp.sum(x * x, axis=1, keepdims=True)
        lane = lax.broadcasted_iota(jnp.int32, (tile, 128), 1)
        v["mom"][i] = jnp.where(lane < 64, one, two)

    weight_copy(1).wait()
    each(tiles, spatial_first)
    for d in range(1, parts):
        moment_copy(d).start()

    batch = 2 if store_count % 2 == 0 else 1
    passage = keys.shape[1]

    def project(i):
        for c in range(batch):
            store_copy(i * batch + c).wait()
        rows = [normed_rows(v["st"][i * batch + c], store_gain[...]) for c in range(batch)]
        rows = jnp.concatenate(rows, axis=0)
        k = jnp.dot(rows, w_ref[2], preferred_element_type=f32).astype(bf16)
        x = jnp.dot(rows, w_ref[3], preferred_element_type=f32)
        for c in range(batch):
            at = slice(c * passage, (c + 1) * passage)
            keys[i * batch + c] = k[at]
            values_t[i * batch + c] = x[at].T.astype(bf16)

    def spatial_rest():
        for d in range(1, parts):
            moment_copy(d).wait_recv()
        weight_copy(4).wait()
        weight_copy(5).wait()

        def one(i):
            mom = v["mom"][i]
            for d in range(1, parts):
                mom = mom + v["mom_in"][d - 1, i]
            mom = mom / (width * parts)
            mean = mom[:, 0:1]
            spread = mom[:, 64:65] - mean * mean
            x = (v["spatial"][i] - mean) * lax.rsqrt(spread + norm_eps) * spatial_gain[...]
            x = x.astype(bf16)
            bias = jnp.concatenate([bias_ref[...]] * (-(-8 // heads)), axis=0).T
            mixed = [
                jnp.dot(mix_ref[h], x[:, h * dim : (h + 1) * dim], preferred_element_type=f32)
                + bias[:, h : h + 1]
                for h in range(heads)
            ]
            mixed = jnp.concatenate(mixed, axis=1)
            carry = jnp.dot(normed[i], w_ref[4], preferred_element_type=f32)
            v["gated"][i] = erf_gelu(carry) * mixed
            v["blend"][i] = jax.nn.sigmoid(jnp.dot(normed[i], w_ref[5], preferred_element_type=f32))

        each(tiles, one)

    def attend(queries, passages, put):
        for c in range(cap):
            v["s"][c] = (
                lax.dot_general(
                    keys[passages[c]],
                    stacked_queries(queries[c], heads),
                    (((1,), (1,)), ((), ())),
                    preferred_element_type=f32,
                )
                * scale
            )
        totals = []
        levels = []
        for c in range(cap):
            s = v["s"][c]
            peak = jnp.max(s, axis=0, keepdims=True)
            w = jnp.exp(s - peak)
            total = jnp.sum(w, axis=0, keepdims=True)
            v["p"][c] = w.astype(bf16)
            totals.append(total)
            levels.append(peak + jnp.log(total))
        for c in range(cap):
            o = jnp.dot(values_t[passages[c]], v["p"][c], preferred_element_type=f32)
            put(c, (own_head(o, heads) / totals[c]).astype(bf16), levels[c])

    def send_results(s, j):
        for copy in result_copies(s, j):
            copy.start()

    def attention(s, send=True):
        mine = me * cap

        def for_mate(j):
            query_copy(s, j).wait_recv()

            def put(c, value, level):
                rout[s, j, c] = value
                lout[s, j, c] = level

            attend([qin[s, j, c] for c in range(cap)], [look(s, j, mine + c) for c in range(cap)], put)
            if send:

                @pl.when(j > 1)
                def _():
                    send_results(s, j - 1)

        each(plane, for_mate, 1)

        def put_here(c, value, level):
            rin[s][p * cap + c] = value
            lin[s][p * cap + c] = level

        here = [block(s)[look(s, 0, section + mine + c)] for c in range(cap)]
        if send and plane > 1:
            send_results(s, plane - 1)
        attend(here, [look(s, 0, mine + c) for c in range(cap)], put_here)

    def source(s, span, k):
        i = look(s, 0, 2 * section + span * picks + k) - base
        return jnp.clip(i, 0, local - 1), (i >= 0) & (i < local)

    def weigh(s, h, more):
        def one(i):
            for k in range(picks):
                at, inside = source(s, h * group + i, k)
                v["lev"][k, pl.ds(i, 1)] = jnp.where(inside, lin[s][at], far)

        unrolled(group, one)
        levels = [v["lev"][k] for k in range(picks)] + more
        top = functools.reduce(jnp.maximum, levels)
        ws = [jnp.exp(level - top) for level in levels]
        total = sum(ws)
        for k, w in enumerate(ws):
            v["wt"][k] = w / total
        return top + jnp.log(total)

    def summed(s, h, i, more):
        at = pl.ds(i, 1)
        terms = [v["wt"][k, at] * rin[s][source(s, h * group + i, k)[0]].astype(f32) for k in range(picks)]
        for k, ref in enumerate(more):
            terms.append(v["wt"][picks + k, at] * ref[i].astype(f32))
        return sum(terms)

    def wait_results(s):
        def one(j):
            for copy in result_copies(s, j):
                copy.wait_recv()

        each(plane, one, 1)

    def arrived(s, h):
        if (s if s else columns) < 2:
            return [], []
        i = (s if s else columns) - 2
        for copy in merged_copies(i + 1, h):
            copy.wait_recv()
        return [mlin[i, h]], [mid.at[i, h]]

    def merge(s):
        wait_results(s)
        for d in range(1, halves + 1):
            h = lax.rem(side + d, halves)
            levels, blocks = arrived(s, h)
            mlout[s - 1, h] = weigh(s, h, levels)

            def one(i):
                mout[s - 1, h, i] = summed(s, h, i, blocks).astype(bf16)

            unrolled(group, one)
            for copy in merged_copies(s, h):
                copy.start()

    own_copy.wait()
    weight_copy(2).wait()
    weight_copy(3).wait()
    cuts = [store_count // batch * part // 12 for part in (0, 1, 4, 7, 10, 12)]
    if columns == 1:
        each(store_count // batch, project)
    for s in range(1, columns):
        for h in range(halves):
            k = (s - 1) * halves + h
            if k + 1 < len(cuts):
                each(cuts[k + 1], project, cuts[k])
            if k == 0:
                each(n, lambda d: tab_copy(d).wait_recv(), 1)
                to_smem = pltpu.make_async_copy(tabs_v, tabs_s, v["loc"].at[1])
                to_smem.start()
                to_smem.wait()
            if s == columns - 1 and h == 0:
                for done in range(1, s - 1):
                    attention(done)
            ring_copy(s - 1, h).wait_recv()
            if s < columns - 1:
                ring_copy(s, h).start()
        select(s)
    spatial_rest()
    if columns > 1:
        attention(columns - 2)
    for s in range(1, columns - 1):
        merge(s)
        if s == 1:
            attention(0, False)
            attention(columns - 1)
            each(plane, lambda j: send_results(0, j), 1)
    if columns > 1:
        merge(columns - 1)
    wait_results(0)

    lanes = pl.ds(pl.multiple_of(side * width, width), width)

    def final(h, to):
        levels, blocks = arrived(0, h)
        weigh(0, h, levels)

        def one(i):
            span = h * group + i
            memory = summed(0, h, i, blocks).T
            memory = jnp.concatenate([memory[c * length : (c + 1) * length] for c in range(heads)], axis=1)
            at = pl.ds(pl.multiple_of(lax.rem(span, per) * length, length), length)
            t = span // per
            to(i, (v["gated"][t, at] + v["blend"][t, at] * memory).astype(bf16))

        unrolled(group, one)

    def half_copy(d):
        i = d - 1
        return remote(half.at[i], out_ref.at[:, lanes], v["ts"].at[i], v["tr"].at[i], other(d))

    def rows_of(i):
        return pl.ds(pl.multiple_of(i * length, length), length)

    for d in range(1, parts):

        def keep(i, value):
            half[d - 1, rows_of(i)] = value

        final(lax.rem(side + d, parts), keep)
        half_copy(d).start()

    def keep_own(i, value):
        out_ref[rows_of(i), lanes] = value

    final(side, keep_own)

    for d in range(1, parts):
        half_copy(d).wait()
        moment_copy(d).wait_send()
    each(n, lambda d: tab_copy(d).wait_send(), 1)
    for s in range(columns - 1):
        for h in range(halves):
            ring_copy(s, h).wait_send()
    for s in range(columns):

        def done(j):
            query_copy(s, j).wait_send()
            for copy in result_copies(s, j):
                copy.wait_send()

        each(plane, done, 1)
    for s in range(1, columns):
        for h in range(halves):
            for copy in merged_copies(s, h):
                copy.wait_send()


def per_device(
    tokens,
    route_ids,
    store,
    token_gain,
    store_gain,
    carry_weight,
    spatial_weight,
    spatial_gain,
    position_mix,
    position_bias,
    query_weight,
    key_weight,
    read_weight,
    blend_weight,
    output_weight,
):
    row_count, model = tokens.shape
    local_heads, block_length = position_mix.shape[:2]
    width = carry_weight.shape[1]
    head_dim = width // local_heads
    span_count, pick_count = route_ids.shape
    span_length = row_count // span_count
    store_count, passage_length = store.shape[:2]
    owner_count = lax.axis_size("st")
    requests = span_count * pick_count
    cap = max(1, 2 * requests // owner_count)
    slots = owner_count * cap

    parts = lax.axis_size("tp")
    columns = 4 if owner_count % 4 == 0 else 1
    plane = owner_count // columns
    local = plane * cap
    wide = local_heads * span_length
    tiles = row_count // block_length
    halves = parts
    group = span_count // halves
    tab_size = 2 * (-(-owner_count * cap // 128) * 128) + (-(-requests // 128) * 128)
    vmem = pl.BlockSpec(memory_space=pltpu.VMEM)
    hbm = pl.BlockSpec(memory_space=pltpu.HBM)
    dma = pltpu.SemaphoreType.DMA
    V = pltpu.VMEM
    in_hbm = lambda x: pltpu.with_memory_space_constraint(x, pltpu.HBM)
    scratch = dict(
        tok=V((tiles, block_length, model), bf16),
        normed=V((tiles, block_length, model), bf16),
        st=V((store_count, passage_length, model), bf16),
        w=V((6, model, width), bf16),
        keys=V((store_count, passage_length, width), bf16),
        values_t=V((store_count, width, passage_length), bf16),
        spatial=V((tiles, block_length, width), f32),
        gated=V((tiles, block_length, width), f32),
        blend=V((tiles, block_length, width), f32),
        mom=V((tiles, block_length, 128), f32),
        mom_in=V((parts, tiles, block_length, 128), f32),
        small=[
            V((pick_count, span_count), jnp.int32),
            V((1, model), f32),
            V((1, model), f32),
            V((1, width), f32),
            V((local_heads, block_length), f32),
            V((local_heads, block_length, block_length), bf16),
        ],
        small_sem=dma((6,)),
        tab=V((1, tab_size), jnp.int32),
        own_tab=pltpu.SMEM((1, tab_size), jnp.int32),
        tabs_v=V((owner_count, 1, tab_size), jnp.int32),
        tabs_s=pltpu.SMEM((owner_count, 1, tab_size), jnp.int32),
        q_own=V((span_count, span_length, width), bf16),
        qcol=[V((span_count, span_length, width), bf16)] * (columns - 1),
        qout=V((columns, plane, cap, span_length, width), bf16),
        qin=V((columns, plane, cap, span_length, width), bf16),
        rout=V((columns, plane, cap, head_dim, wide), bf16),
        lout=V((columns, plane, cap, 1, wide), f32),
        rin=[V((local, head_dim, wide), bf16)] * columns,
        lin=[V((local, 1, wide), f32)] * columns,
        mout=V((columns, halves, group, head_dim, wide), bf16),
        mlout=V((columns, halves, group, wide), f32),
        mid=V((columns, halves, group, head_dim, wide), bf16),
        mlin=V((columns, halves, group, wide), f32),
        lev=V((pick_count, group, wide), f32),
        wt=V((pick_count + 1, group, wide), f32),
        half=V((parts, row_count // parts, width), bf16),
        s=V((cap, passage_length, wide), f32),
        p=V((cap, passage_length, wide), bf16),
        tok_sem=dma((tiles,)),
        st_sem=dma((store_count,)),
        w_sem=dma((6,)),
        loc=dma((3,)),
        tab_send=dma((owner_count,)),
        tab_recv=dma((owner_count,)),
        ring_send=dma((columns, halves)),
        ring_recv=dma((columns, halves)),
        **{name: dma((columns, plane)) for name in ("qs", "qr", "rs", "rr", "ls", "lr")},
        **{name: dma((columns, halves)) for name in ("ms", "mr", "mls", "mlr")},
        **{name: dma((parts,)) for name in ("ts", "tr", "xs", "xr")},
    )
    by_rows = pl.pallas_call(
        functools.partial(layer_kernel, (columns, plane, parts, local_heads, cap, pick_count, halves)),
        in_specs=[hbm] * 14,
        out_specs=vmem,
        out_shape=jax.ShapeDtypeStruct((row_count // parts, parts * width), bf16),
        scratch_shapes=[scratch],
        compiler_params=pltpu.CompilerParams(
            collective_id=0, has_side_effects=True, vmem_limit_bytes=53 * 2**20
        ),
        name="layer",
    )(
        in_hbm(route_ids.T),
        in_hbm(token_gain.reshape(1, model)),
        in_hbm(store_gain.reshape(1, model)),
        in_hbm(spatial_gain.reshape(1, width)),
        in_hbm(position_bias),
        in_hbm(position_mix),
        tokens,
        store,
        query_weight,
        spatial_weight,
        key_weight,
        read_weight,
        carry_weight,
        blend_weight,
    )
    return jnp.dot(by_rows, output_weight, preferred_element_type=f32).astype(bf16)


def solution(mesh):
    in_specs = (
        P("st", None),
        P("st", None),
        P("st", None, None),
        P(),
        P(),
        P(None, "tp"),
        P(None, "tp"),
        P("tp"),
        P("tp", None, None),
        P("tp", None),
        P(None, "tp"),
        P(None, "tp"),
        P(None, "tp"),
        P(None, "tp"),
        P(),
    )
    out_specs = P(("st", "tp"), None)
    return jax.shard_map(
        per_device, mesh=mesh, in_specs=in_specs, out_specs=out_specs, check_vma=False
    )
```
